256 devices in a mesh: sp: 16 (over y, x), dp: 16 (over z, core).
Axes of the slice: x: 4, y: 4, z: 8, core: 2. Of those that a mesh axis runs over, the one named last changes fastest.
Arguments:
- tokens: bfloat16 [16, 4096, 2048], P('dp', 'sp'), may hold values from -6 to 6
- key_weight: bfloat16 [2048, 2048], P('dp'), may hold values from -0.125 to 0.125
- queries: bfloat16 [16, 4096, 16, 128], P('dp', None, 'sp'), may hold values from -1.5 to 1.5
- values: bfloat16 [16, 4096, 16, 256], P('dp', None, 'sp'), may hold values from -1.5 to 1.5
- cotangent: bfloat16 [16, 4096, 4096], P('dp', 'sp'), may hold values from -6 to 6
- log_decay: float32 [16], replicated, may hold values from -0.034 to 0, as said below
Outputs:
- grad_tokens: bfloat16 [16, 4096, 2048], P('dp', 'sp')
- grad_queries: bfloat16 [16, 4096, 16, 128], P('dp', None, 'sp')
- grad_values: bfloat16 [16, 4096, 16, 256], P('dp', None, 'sp')
- grad_key_weight: float32 [2048, 2048], P('dp')
The draws below stay inside these ranges and needn't reach their ends.
Inputs may be any that keep to these rules, and one draw needn't show every extreme that they name: `log_decay`: every entry is below zero.
All inputs are finite; a program needn't handle non-finite values.
Results may differ from the reference program's by a relative error of at most 0.0075.
Values may be sent and summed in bfloat16 or wider, within the bound.
A program may use at most 128 MiB of HBM per device.

```python
import jax
import jax.numpy as jnp
from jax import lax

D = 2048
HEADS = 16
KEY_DIM = 128
VALUE_DIM = 256
BLOCK = 128
LENGTH = 4096
SEQS = 16


def draw_log_decay(key, part):
    ranking = jax.random.permutation(jax.random.fold_in(key, 11), HEADS)
    fast_count = HEADS // 2
    spread = jax.random.uniform(jax.random.fold_in(key, 12), (HEADS,), jnp.float32)
    slow_rate = jnp.minimum(jnp.exp(jnp.log(0.2 / LENGTH) + spread * jnp.log(10.0)), 0.01)
    fast_rate = jnp.exp(jnp.log(0.01) + spread * jnp.log(100.0 / 30.0))
    return -jnp.where(ranking < fast_count, fast_rate, slow_rate).astype(jnp.float32)


def raised(result, rng, source, target, shards_of, factor):
    def block_of(dim):
        return (jnp.arange(result.shape[dim]) // (result.shape[dim] // shards_of)).reshape((-1,) + (1,) * (result.ndim - 1 - dim))

    first = jax.random.permutation(rng, shards_of)[block_of(target)]
    second = (block_of(target) + shards_of // 2) % shards_of
    return jnp.where((block_of(source) == first) | (block_of(source) == second), factor * result, result)


def block_scale(own_key, shape, shards, smallest, high):
    gain, own = 1.0, jax.random.fold_in(own_key, 6)
    for axis_at, shards_of in shards:
        heights = jnp.exp(jax.random.uniform(jax.random.fold_in(own, axis_at), (shards_of,), jnp.float32, smallest / len(shards), high / len(shards)))
        gain = gain * jnp.repeat(heights, shape[axis_at] // shards_of).reshape([-1 if axis == axis_at else 1 for axis in range(len(shape))])
    return gain


def gaussian(key, shape, scale, reach, pieces=(), kind=jnp.bfloat16):
    factor_of = block_scale(key, shape, pieces, -0.22, 0.18) if pieces else 1.0
    result = jax.random.normal(key, shape, jnp.float32) * scale * factor_of
    return jnp.minimum(jnp.maximum(result, -reach), reach).astype(kind)


def bell_draw_with(stream_key, extent, deviation, bound, pieces, heavy, kind=jnp.bfloat16):
    result = deviation * jax.random.normal(stream_key, extent, jnp.float32)
    if pieces:
        result = result * block_scale(stream_key, extent, pieces, -0.22, 0.18)
    return jnp.clip(raised(result, jax.random.fold_in(stream_key, 3), *heavy), -bound, bound).astype(kind)


def setup_inputs(seed: int = 0) -> dict:
    arg_keys = jax.random.split(jax.random.key(seed), 7)
    tokens = gaussian(arg_keys[0], (SEQS, LENGTH, D), 1.0, 6.0, ((0, 16), (1, 16)))
    key_weight = gaussian(arg_keys[1], (HEADS * KEY_DIM, D), D ** -0.5, 0.125, ((0, 16),))
    queries = gaussian(arg_keys[2], (SEQS, LENGTH, HEADS, KEY_DIM), 0.1, 1.5, ((0, 16), (2, 16)))
    values = gaussian(arg_keys[3], (SEQS, LENGTH, HEADS, VALUE_DIM), 0.1, 1.5, ((0, 16), (2, 16)))
    cotangent = bell_draw_with(arg_keys[4], (SEQS, LENGTH, HEADS * VALUE_DIM), 1.0, 6.0, ((0, 16), (1, 16)), (0, 2, 16, 2.0))
    log_decay = draw_log_decay(jax.random.fold_in(arg_keys[6], 71), 0)
    return {"tokens": tokens, "key_weight": key_weight, "queries": queries, "values": values, "cotangent": cotangent, "log_decay": log_decay}


def product(form, left, right):
    return jnp.einsum(form, left.astype(jnp.float32), right.astype(jnp.float32))


def rotation(seq_len, half):
    position = jnp.arange(seq_len, dtype=jnp.float32)
    frequency = 10000.0 ** (-jnp.arange(half, dtype=jnp.float32) / half)
    angle = position[:, None] * frequency[None, :]
    return jnp.cos(angle)[:, None, :], jnp.sin(angle)[:, None, :]


def rotate(vectors, cosine, sine):
    half = vectors.shape[-1] // 2
    front, back = vectors[..., :half], vectors[..., half:]
    return jnp.concatenate([front * cosine - back * sine, front * sine + back * cosine], axis=-1)


def unrotate(grads, cosine, sine):
    half = grads.shape[-1] // 2
    front, back = grads[..., :half], grads[..., half:]
    return jnp.concatenate([front * cosine + back * sine, back * cosine - front * sine], axis=-1)


def retention_backward(query_rows, key_rows, value_rows, cotan_rows, head_decay):
    seq_len, heads_here, key_width = query_rows.shape
    nblocks = seq_len // BLOCK
    cosine, sine = rotation(seq_len, key_width // 2)
    factor = key_width ** -0.5
    rot_query = rotate(query_rows.astype(jnp.float32), cosine, sine).astype(jnp.bfloat16)
    rot_key = (rotate(key_rows.astype(jnp.float32), cosine, sine) * factor).astype(jnp.bfloat16)

    def blocks(array):
        return array.reshape(nblocks, BLOCK, heads_here, array.shape[-1])

    block_query, block_key = blocks(rot_query), blocks(rot_key)
    block_value, block_cotan = blocks(value_rows), blocks(cotan_rows)
    inside = jnp.arange(BLOCK, dtype=jnp.float32)
    offset = inside[:, None] - inside[None, :]
    within = jnp.where(offset[None] >= 0, jnp.exp(jnp.maximum(offset, 0.0)[None] * head_decay[:, None, None]), 0.0)
    rising = jnp.exp((inside + 1.0)[:, None] * head_decay[None, :])[None, :, :, None]
    falling = jnp.exp((BLOCK - 1.0 - inside)[:, None] * head_decay[None, :])[None, :, :, None]
    scores = (product("nihd,njhd->nhij", block_query, block_key) * within[None]).astype(jnp.bfloat16)
    mixing = (product("nihe,njhe->nhij", block_cotan, block_value) * within[None]).astype(jnp.bfloat16)
    decayed_queries = (block_query.astype(jnp.float32) * rising).astype(jnp.bfloat16)
    decayed_keys = (block_key.astype(jnp.float32) * falling).astype(jnp.bfloat16)
    block_states = product("nihd,nihe->nhde", decayed_keys, block_value)
    block_trails = product("nihd,nihe->nhde", decayed_queries, block_cotan)
    block_index = jnp.arange(nblocks, dtype=jnp.float32)
    spacing = block_index[:, None] - block_index[None, :] - 1.0
    earlier = jnp.where(spacing[None] >= 0,
                        jnp.exp(jnp.maximum(spacing, 0.0)[None] * BLOCK * head_decay[:, None, None]), 0.0)
    later = jnp.transpose(earlier, (0, 2, 1))
    entering = jnp.einsum("hnm,mhde->nhde", earlier, block_states,
                          precision=lax.Precision.HIGHEST).astype(jnp.bfloat16)
    trailing = jnp.einsum("hnm,mhde->nhde", later, block_trails,
                          precision=lax.Precision.HIGHEST).astype(jnp.bfloat16)
    grad_rq = product("nhij,njhd->nihd", mixing, block_key) + rising * product("nihe,nhde->nihd", block_cotan, entering)
    grad_rk = product("nhij,nihd->njhd", mixing, block_query) + falling * product("nihe,nhde->nihd", block_value, trailing)
    grad_value = product("nhij,nihe->njhe", scores, block_cotan) + falling * product("nihd,nhde->nihe", block_key, trailing)
    grad_rq = grad_rq.reshape(seq_len, heads_here, key_width)
    grad_rk = grad_rk.reshape(seq_len, heads_here, key_width)
    grad_query = unrotate(grad_rq, cosine, sine).astype(jnp.bfloat16)
    grad_key = (unrotate(grad_rk, cosine, sine) * factor).astype(jnp.bfloat16)
    grad_value = grad_value.reshape(seq_len, heads_here, -1).astype(jnp.bfloat16)
    return grad_query, grad_key, grad_value


def reference(tokens, key_weight, queries, values, cotangent, log_decay):
    seq_len = tokens.shape[1]

    def one_sequence(weight_sum, item):
        token_rows, query_rows, value_rows, cotan_rows = item
        key_proj = jnp.dot(token_rows, key_weight.T, preferred_element_type=jnp.float32).astype(jnp.bfloat16)
        grad_query, grad_key, grad_value = retention_backward(
            query_rows, key_proj.reshape(seq_len, HEADS, KEY_DIM), value_rows,
            cotan_rows.reshape(seq_len, HEADS, VALUE_DIM), log_decay)
        key_grads = grad_key.reshape(seq_len, HEADS * KEY_DIM)
        grad_token = jnp.dot(key_grads, key_weight, preferred_element_type=jnp.float32).astype(jnp.bfloat16)
        weight_sum = weight_sum + jnp.dot(key_grads.T, token_rows, preferred_element_type=jnp.float32)
        return weight_sum, (grad_token, grad_query, grad_value)

    start_sum = jnp.zeros((HEADS * KEY_DIM, D), jnp.float32)
    weight_grad, outputs = lax.scan(one_sequence, start_sum, (tokens, queries, values, cotangent))
    return outputs[0], outputs[1], outputs[2], weight_grad
```

```python
import functools

import jax
import jax.numpy as jnp
import numpy as np
from jax import lax
from jax.experimental import pallas as pl
from jax.experimental.pallas import tpu as pltpu
from jax.sharding import PartitionSpec as P

MESH = pl.DeviceIdType.MESH
F32, BF16 = jnp.float32, jnp.bfloat16
BLOCK = 128
NB = 32
WIDTH = 2048
C1 = 1280
CH = C1 // 2
C2 = WIDTH - C1
FACTOR = BLOCK**-0.5


def tables():
    half = 64
    freq = 10000.0 ** (-np.arange(half, dtype=np.float64) / half)
    freq = np.concatenate([freq, freq])
    sign = np.where(np.arange(128) < half, -1.0, 1.0)
    ang_j = np.arange(128, dtype=np.float64)[:, None] * freq
    ang_n = 128.0 * np.arange(NB, dtype=np.float64)[:, None] * freq
    inside = np.stack([np.cos(ang_j), np.sin(ang_j), sign * np.cos(ang_j), sign * np.sin(ang_j)])
    across = np.stack([np.cos(ang_n), np.sin(ang_n)], axis=1)
    return inside.astype(np.float32), across.astype(np.float32)


def dot(a, b, ca, cb):
    return lax.dot_general(a, b, (((ca,), (cb,)), ((), ())), preferred_element_type=F32)


SCRATCH = dict(
    tok=((512, WIDTH), BF16),
    wall=((8, 128, WIDTH), BF16),
    vv=((NB, 128, 256), BF16),
    rq=((NB, 128, 128), BF16),
    dq=((NB, 128, 128), BF16),
    cosv=((NB, 128, 128), F32),
    sinv=((NB, 128, 128), F32),
    jtv=((4, 128, 128), F32),
    ntv=((NB, 2, 128), F32),
    within=((128, 128), F32),
    rise=((128, 128), F32),
    fall=((128, 128), F32),
    cot=((NB, 128, 256), BF16),
    mix=((NB, 128, 128), BF16),
    trl=((NB, 128, 256), F32),
    trb=((NB, 128, 256), BF16),
    gko=((NB, 128, 128), BF16),
    gki=((4, 128, 1024), BF16),
    keyo=((8, 4, 128, 128), BF16),
    keyi=((NB, 128, 128), BF16),
    ent=((128, 256), F32),
    gts=((256, WIDTH), BF16),
    gtr=((256, WIDTH), BF16),
    gtb=((256, WIDTH), BF16),
    gqb=((NB, 128, 128), BF16),
    gvb=((NB, 128, 256), BF16),
    dwz=((8, 128, C1), BF16),
    rz=((2, 7, 128, CH), BF16),
    dwx=((16, 8, 8, C2), BF16),
    rx=((16, 8, 8, C2), BF16),
    zx=((8, 8, C2), BF16),
    zr=((8, 8, C2), BF16),
    px=((16, 8, C1), BF16),
    pr=((16, 8, C1), BF16),
    fin=((16, 8, WIDTH), BF16),
    dwo=((16, 8, WIDTH), F32),
)
SEMS = dict(
    loc=6, cot_s=16, cot_r=16, tok_s=1, tok_r=1, wp_s=4, wp_r=4, wm_s=4, wm_r=4, gk_s=16, gk_r=16, key_s=16, key_r=16,
    gt_s=1, gt_r=1, rz_s=14, rz_r=14, rx_s=16, rx_r=16, zx_s=8, zx_r=8, px_s=16, px_r=16, fin_s=16, fin_r=16, out=4,
)


def kernel(ld_ref, jt_ref, nt_ref, tok_ref, w_ref, q_ref, v_ref, cot_ref, gt_o, gq_o, gv_o, dw_o, *scratch):
    s = dict(zip([*SCRATCH, *SEMS], scratch, strict=True))
    B = type("B", (), s)
    sp, dp = lax.axis_index("sp"), lax.axis_index("dp")
    y, x = lax.div(sp, 4), lax.rem(sp, 4)
    z, c = lax.div(dp, 2), lax.rem(dp, 2)
    head_core = lax.rem(x, 2)
    head_at = lax.div(sp, 2)

    def plane(t):
        def off(u):
            return lax.rem(2 + u + lax.div(u, 2) + 2 * lax.div(u, 3), 4)

        dy, dx = off(lax.div(t, 4)), off(lax.rem(t, 4))
        to = lax.rem(y + dy, 4) * 4 + lax.rem(x + dx, 4)
        of = lax.rem(y + 4 - dy, 4) * 4 + lax.rem(x + 4 - dx, 4)
        return to, of

    def zdev(dz, core=c):
        return lax.rem(z + 8 + dz, 8) * 2 + core

    def remote(src, dst, ss, rs, dev):
        return pltpu.make_async_remote_copy(
            src_ref=src, dst_ref=dst, send_sem=ss, recv_sem=rs, device_id=dev, device_id_type=MESH
        )

    def arrived(ref, sem):
        pltpu.make_async_copy(ref, ref, sem).wait()

    def loop(lo, hi, f):
        def step(i, carry):
            f(i)
            return carry

        lax.fori_loop(lo, hi, step, 0)

    bar = pltpu.get_barrier_semaphore()
    partner = (sp, zdev(0, 1 - c))

    def greet(k):
        for core in (c, 1 - c):
            pl.semaphore_signal(bar, inc=1, device_id=(lax.rem(sp + k, 16), zdev(0, core)), device_id_type=MESH)

    def greet_z(k):
        pl.semaphore_signal(bar, inc=1, device_id=(sp, zdev(k)), device_id_type=MESH)

    loads = [
        pltpu.make_async_copy(q_ref, B.rq, B.loc.at[0]),
        pltpu.make_async_copy(v_ref, B.vv, B.loc.at[1]),
        pltpu.make_async_copy(tok_ref, B.tok.at[pl.ds(c * 256, 256)], B.loc.at[2]),
        pltpu.make_async_copy(w_ref, B.wall.at[z], B.loc.at[3]),
        pltpu.make_async_copy(jt_ref, B.jtv, B.loc.at[4]),
        pltpu.make_async_copy(nt_ref, B.ntv, B.loc.at[5]),
    ]
    for cp in loads:
        cp.start()
    own_cot = pltpu.make_async_copy(
        cot_ref.at[:, :, pl.ds(pl.multiple_of(sp * 256, 256), 256)], B.cot.at[pl.ds(2 * sp, 2)], B.cot_r.at[sp]
    )
    own_cot.start()

    loop(1, 16, greet)
    pl.semaphore_signal(bar, inc=1, device_id=partner, device_id_type=MESH)
    loop(1, 8, greet_z)
    pl.semaphore_wait(bar, 38)

    up, down = (sp, zdev(1)), (sp, zdev(-1))
    w_up = remote(w_ref, B.wall.at[z], B.wp_s.at[0], B.wp_r.at[0], up)
    w_down = remote(w_ref, B.wall.at[z], B.wm_s.at[0], B.wm_r.at[0], down)
    w_up.start()
    w_down.start()

    def cot_copy(t):
        to, _ = plane(t)
        return remote(
            cot_ref.at[:, :, pl.ds(pl.multiple_of(to * 256, 256), 256)],
            B.cot.at[pl.ds(2 * sp, 2)],
            B.cot_s.at[t],
            B.cot_r.at[sp],
            (to, dp),
        )

    loop(0, 15, lambda t: cot_copy(t).start())
    tok_copy = remote(tok_ref, B.tok.at[pl.ds(c * 256, 256)], B.tok_s.at[0], B.tok_r.at[0], partner)
    tok_copy.start()

    ld = ld_ref[sp]
    rows = lax.broadcasted_iota(jnp.int32, (128, 128), 0).astype(F32)
    cols = lax.broadcasted_iota(jnp.int32, (128, 128), 1).astype(F32)
    offset = rows - cols
    B.within[...] = jnp.where(offset >= 0, jnp.exp(jnp.maximum(offset, 0.0) * ld), 0.0)
    B.rise[...] = jnp.exp((rows + 1.0) * ld)
    B.fall[...] = jnp.exp((127.0 - rows) * ld)
    growth = jnp.exp(jnp.full((1, 256), 128.0, F32) * ld)
    loads[4].wait()
    loads[5].wait()
    loads[0].wait()

    def turn(n):
        cn, sn = B.ntv[n, 0:1, :], B.ntv[n, 1:2, :]
        cosine = cn * B.jtv[0] - sn * B.jtv[1]
        sine = sn * B.jtv[2] + cn * B.jtv[3]
        B.cosv[n] = cosine
        B.sinv[n] = sine
        u = B.rq[n].astype(F32)
        r = (u * cosine + pltpu.roll(u, 64, 1) * sine).astype(BF16)
        B.rq[n] = r
        B.dq[n] = (r.astype(F32) * B.rise[...]).astype(BF16)

    loop(0, NB, turn)

    def keys(hh):
        def part(i):
            k = dot(B.tok[pl.ds(pl.multiple_of(i * 256, 256), 256), :], B.wall[hh], 1, 1)
            B.keyo[hh, pl.ds(2 * i, 2)] = k.astype(BF16).reshape(2, 128, 128)

        loop(0, 2, part)

    def zat(dz):
        return lax.rem(z + 8 + dz, 8)

    loads[2].wait()
    arrived(B.tok.at[pl.ds((1 - c) * 256, 256)], B.tok_r.at[0])
    loads[3].wait()

    def w_forward(k, rows_up, rows_down):
        a, b = zat(-k), zat(k)
        arrived(B.wall.at[a], B.wp_r.at[k - 1])
        fu = remote(B.wall.at[a, rows_up], B.wall.at[a, rows_up], B.wp_s.at[k], B.wp_r.at[k], up)
        fu.start()
        arrived(B.wall.at[b], B.wm_r.at[k - 1])
        fd = remote(B.wall.at[b, rows_down], B.wall.at[b, rows_down], B.wm_s.at[k], B.wm_r.at[k], down)
        fd.start()
        return fu, fd

    full = pl.ds(0, 128)

    def cot_chunk(t):
        _, p = plane(t)
        arrived(B.cot.at[pl.ds(2 * p, 2)], B.cot_r.at[p])
        for b in range(2):
            n = 2 * p + b
            cb = B.cot[n]
            m = dot(cb, B.vv[n], 1, 1) * B.within[...]
            B.mix[n] = m.astype(BF16)
            B.trl[n] = dot(B.dq[n], cb, 0, 0)

    loads[1].wait()
    f1 = w_forward(1, full, full)
    loop(0, 3, lambda i: keys(zat(i - 1)))
    loop(0, 8, cot_chunk)
    f2 = w_forward(2, full, full)
    loop(0, 2, lambda i: keys(zat(4 * i - 2)))
    loop(8, 16, cot_chunk)

    def scan(i, carry):
        n = NB - 1 - i
        B.trb[n] = carry.astype(BF16)
        return B.trl[n] + growth * carry

    lax.fori_loop(0, NB, scan, jnp.zeros((128, 256), F32))

    def gk_copy(t):
        to, _ = plane(t)
        return remote(
            B.gko.at[pl.ds(2 * to, 2)],
            B.gki.at[pl.ds(2 * c, 2), :, pl.ds(pl.multiple_of(head_at * 128, 128), 128)],
            B.gk_s.at[t],
            B.gk_r.at[head_at * 2 + c],
            (to, zdev(0, head_core)),
        )

    def gk_chunk(t):
        p, _ = plane(t)
        for b in range(2):
            n = 2 * p + b
            g = dot(B.mix[n], B.rq[n], 0, 0) + B.fall[...] * dot(B.vv[n], B.trb[n], 1, 1)
            g = g * B.cosv[n] - pltpu.roll(g, 64, 1) * B.sinv[n]
            B.gko[n] = (g * FACTOR).astype(BF16)

    def gk_step(t):
        gk_chunk(t)
        gk_copy(t).start()

    loop(0, 15, gk_step)
    gk_chunk(15)

    @pl.when(head_core == c)
    def _():
        pltpu.make_async_copy(
            B.gko.at[pl.ds(2 * sp, 2)],
            B.gki.at[pl.ds(2 * c, 2), :, pl.ds(pl.multiple_of(head_at * 128, 128), 128)],
            B.gk_r.at[head_at * 2 + c],
        ).start()

    @pl.when(head_core != c)
    def _():
        gk_copy(15).start()

    f3 = w_forward(3, pl.ds(0, 64), pl.ds(64, 64))
    loop(0, 2, lambda i: keys(zat(6 * i - 3)))

    def key_copy(hh, i):
        return remote(
            B.keyo.at[hh, pl.ds(2 * i, 2)],
            B.keyi.at[pl.ds(2 * sp, 2)],
            B.key_s.at[2 * hh + i],
            B.key_r.at[sp],
            (2 * hh + c, zdev(0, i)),
        )

    def key_send(hh):
        for i in range(2):
            mine = jnp.logical_and(2 * hh + c == sp, c == i)

            @pl.when(mine)
            def _():
                pltpu.make_async_copy(
                    B.keyo.at[hh, pl.ds(2 * i, 2)], B.keyi.at[pl.ds(2 * sp, 2)], B.key_r.at[sp]
                ).start()

            @pl.when(jnp.logical_not(mine))
            def _():
                key_copy(hh, i).start()

    loop(0, 7, lambda i: key_send(zat(i - 3)))

    def gki_arrived(i):
        hh, j = lax.div(i, 2), lax.rem(i, 2)
        arrived(B.gki.at[pl.ds(2 * j, 2), :, pl.ds(pl.multiple_of(hh * 128, 128), 128)], B.gk_r.at[i])

    loop(0, 16, gki_arrived)

    def ring_copy(way, half, k):
        slot = (4 - k) if (way == half) else 4 + (3 - k)
        d = zat(k if way == 0 else -k)
        sem = way * 7 + slot
        return remote(
            B.dwz.at[d, :, pl.ds(half * CH, CH)],
            B.rz.at[way, slot],
            B.rz_s.at[sem],
            B.rz_r.at[sem],
            up if way == 0 else down,
        )

    def dw_head(t):
        r, i = lax.rem(t, 2), lax.div(t, 2)
        hh = zat(r * (3 - i) + (1 - r) * (4 + i))
        a = B.gki[:, :, pl.ds(pl.multiple_of(hh * 128, 128), 128)].reshape(512, 128)
        for lo in range(0, WIDTH, 256):
            g = dot(a, B.tok[:, lo : lo + 256], 0, 0)
            if lo < C1:
                B.dwz[hh, :, lo : lo + 256] = g.astype(BF16)
            else:
                B.dwx[:, hh, :, lo - C1 : lo - C1 + 256] = g.reshape(16, 8, 256).astype(BF16)

        @pl.when(t == 0)
        def _():
            ring_copy(0, 0, 4).start()
            ring_copy(1, 1, 4).start()

        @pl.when(t == 1)
        def _():
            ring_copy(0, 1, 3).start()

        @pl.when(t == 2)
        def _():
            ring_copy(1, 0, 3).start()

    loop(0, 8, dw_head)

    def rx_copy(t):
        to, _ = plane(t)
        return remote(B.dwx.at[to], B.rx.at[sp], B.rx_s.at[t], B.rx_r.at[sp], (to, dp))

    loop(0, 15, lambda t: rx_copy(t).start())

    arrived(B.wall.at[zat(4), pl.ds(0, 64)], B.wp_r.at[3])
    arrived(B.wall.at[zat(4), pl.ds(64, 64)], B.wm_r.at[3])
    loop(0, 1, lambda i: keys(zat(4)))
    key_send(zat(4))

    def gt_tile(first):
        def tile(i):
            lo = pl.multiple_of(i * 256, 256)
            j = (1 - c) if first else c
            a = jnp.concatenate([B.gki[2 * j], B.gki[2 * j + 1]], axis=0)
            w = B.wall[:, :, pl.ds(lo, 256)].reshape(1024, 256)
            g = dot(a, w, 1, 0)
            if first:
                B.gts[:, pl.ds(lo, 256)] = g.astype(BF16)
            else:
                B.gtb[:, pl.ds(lo, 256)] = (g + B.gtr[:, pl.ds(lo, 256)].astype(F32)).astype(BF16)

        return tile

    loop(0, 8, gt_tile(True))
    gt_copy = remote(B.gts, B.gtr, B.gt_s.at[0], B.gt_r.at[0], partner)
    gt_copy.start()

    def ring_take(way, half, k):
        slot = (4 - k) if (way == half) else 4 + (3 - k)
        arrived(B.rz.at[way, slot], B.rz_r.at[way * 7 + slot])
        if k == 1:
            return
        d = zat(k - 1 if way == 0 else 1 - k)

        def add(i):
            at = pl.ds(pl.multiple_of(i * 16, 16), 16)
            have = B.dwz[d, at, half * CH : half * CH + CH].astype(F32)
            B.dwz[d, at, half * CH : half * CH + CH] = (have + B.rz[way, slot, at, :].astype(F32)).astype(BF16)

        loop(0, 8, add)
        ring_copy(way, half, k - 1).start()

    ring_take(0, 0, 4)
    ring_take(1, 1, 4)
    arrived(B.gtr, B.gt_r.at[0])
    loop(0, 8, gt_tile(False))
    gt_out = pltpu.make_async_copy(B.gtb, gt_o, B.out.at[0])
    gt_out.start()
    for k in (3,):
        for way in (0, 1):
            for half in (way, 1 - way):
                ring_take(way, half, k)

    def keyi_arrived(p):
        arrived(B.keyi.at[pl.ds(2 * p, 2)], B.key_r.at[p])

    def back(n):
        u = B.keyi[n].astype(F32)
        rk = ((u * B.cosv[n] + pltpu.roll(u, 64, 1) * B.sinv[n]) * FACTOR).astype(BF16)
        cb = B.cot[n]
        sc = (dot(B.rq[n], rk, 1, 1) * B.within[...]).astype(BF16)
        e = B.ent[...]
        g = dot(B.mix[n], rk, 1, 0) + B.rise[...] * dot(cb, e.astype(BF16), 1, 1)
        B.gqb[n] = (g * B.cosv[n] - pltpu.roll(g, 64, 1) * B.sinv[n]).astype(BF16)
        f = B.fall[...]
        gv = dot(sc, cb, 0, 0)
        gt = dot(rk, B.trb[n], 1, 0)
        B.gvb[n, :, 0:128] = (gv[:, 0:128] + f * gt[:, 0:128]).astype(BF16)
        B.gvb[n, :, 128:256] = (gv[:, 128:256] + f * gt[:, 128:256]).astype(BF16)
        dk = (rk.astype(F32) * f).astype(BF16)
        B.ent[...] = dot(dk, B.vv[n], 0, 0) + growth * e

    B.ent[...] = jnp.zeros((128, 256), F32)
    loop(0, 16, keyi_arrived)
    loop(0, 16, back)

    for k in (2,):
        for way in (0, 1):
            for half in (way, 1 - way):
                ring_take(way, half, k)

    def rx_arrived(t):
        _, p = plane(t)
        arrived(B.rx.at[p], B.rx_r.at[p])

    loop(0, 15, rx_arrived)

    def plane_sum(d):
        total = B.dwx[sp, d].astype(F32)

        def more(t, acc):
            _, p = plane(t)
            return acc + B.rx[p, d].astype(F32)

        B.zx[d] = lax.fori_loop(0, 15, more, total).astype(BF16)

    loop(0, 8, plane_sum)

    def zx_copy(k):
        d = zat(k)
        return remote(B.zx.at[d], B.zr.at[z], B.zx_s.at[k], B.zx_r.at[z], (sp, zdev(k)))

    loop(1, 8, lambda k: zx_copy(k).start())

    loop(16, 32, back)
    gq_out = pltpu.make_async_copy(B.gqb, gq_o, B.out.at[1])
    gq_out.start()
    gv_out = pltpu.make_async_copy(B.gvb, gv_o, B.out.at[2])
    gv_out.start()

    for way in (0, 1):
        for half in (way, 1 - way):
            ring_take(way, half, 1)

    def owned(i):
        at = pl.ds(pl.multiple_of(i * 16, 16), 16)
        for half in range(2):
            v = B.dwz[z, at, half * CH : half * CH + CH].astype(F32)
            for way in range(2):
                slot = 3 if way == half else 6
                v += B.rz[way, slot, at, :].astype(F32)
            B.px[pl.ds(2 * i, 2), :, half * CH : half * CH + CH] = v.reshape(2, 8, CH).astype(BF16)

    loop(0, 8, owned)

    def px_copy(t):
        to, _ = plane(t)
        return remote(B.px.at[to], B.pr.at[sp], B.px_s.at[t], B.px_r.at[sp], (to, dp))

    loop(0, 15, lambda t: px_copy(t).start())

    def zr_arrived(k):
        d = zat(k)
        arrived(B.zr.at[d], B.zx_r.at[d])

    loop(1, 8, zr_arrived)
    total = lax.fori_loop(1, 8, lambda k, acc: acc + B.zr[zat(k)].astype(F32), B.zx[z].astype(F32))
    B.fin[sp, :, C1:WIDTH] = total.astype(BF16)

    def pr_arrived(t):
        _, p = plane(t)
        arrived(B.pr.at[p], B.px_r.at[p])

    loop(0, 15, pr_arrived)

    def pr_sum(t, acc):
        _, p = plane(t)
        return acc + B.pr[p].astype(F32)

    B.fin[sp, :, 0:C1] = lax.fori_loop(0, 15, pr_sum, B.px[sp].astype(F32)).astype(BF16)

    def fin_copy(t):
        to, _ = plane(t)
        return remote(B.fin.at[sp], B.fin.at[sp], B.fin_s.at[t], B.fin_r.at[sp], (to, dp))

    loop(0, 15, lambda t: fin_copy(t).start())

    def fin_arrived(t):
        _, p = plane(t)
        arrived(B.fin.at[p], B.fin_r.at[p])

    loop(0, 15, fin_arrived)

    def widen(j):
        B.dwo[j] = B.fin[j].astype(F32)

    loop(0, 16, widen)
    dw_out = pltpu.make_async_copy(B.dwo, dw_o, B.out.at[3])
    dw_out.start()

    for cp in (w_up, w_down, *f1, *f2, *f3, tok_copy, gt_copy):
        cp.wait_send()
    for way in (0, 1):
        for k in (4, 3, 2, 1):
            for half in (0, 1):
                if k < 4 or way == half:
                    ring_copy(way, half, k).wait_send()

    def sent(t):
        cot_copy(t).wait_send()
        gk_copy(t).wait_send()
        rx_copy(t).wait_send()
        px_copy(t).wait_send()
        fin_copy(t).wait_send()

    loop(0, 15, sent)

    @pl.when(head_core != c)
    def _():
        gk_copy(15).wait_send()

    def key_sent(hh):
        for i in range(2):

            @pl.when(jnp.logical_not(jnp.logical_and(2 * hh + c == sp, c == i)))
            def _():
                key_copy(hh, i).wait_send()

    loop(0, 8, key_sent)
    loop(1, 8, lambda k: zx_copy(k).wait_send())
    for cp in (gt_out, gq_out, gv_out, dw_out):
        cp.wait()


def body(tokens, key_weight, queries, values, cotangent, log_decay):
    inside, across = tables()
    any_space = pl.BlockSpec(memory_space=pl.ANY)
    shapes = [
        jax.ShapeDtypeStruct((256, WIDTH), BF16),
        jax.ShapeDtypeStruct((NB, 128, 128), BF16),
        jax.ShapeDtypeStruct((NB, 128, 256), BF16),
        jax.ShapeDtypeStruct((16, 8, WIDTH), F32),
    ]
    gt, gq, gv, dw = pl.pallas_call(
        kernel,
        out_shape=shapes,
        in_specs=[pl.BlockSpec(memory_space=pltpu.SMEM)] + [any_space] * 7,
        out_specs=[any_space] * 4,
        scratch_shapes=[pltpu.VMEM(shape, kind) for shape, kind in SCRATCH.values()]
        + [pltpu.SemaphoreType.DMA((n,)) for n in SEMS.values()],
        compiler_params=pltpu.CompilerParams(
            collective_id=0, has_side_effects=True, vmem_limit_bytes=58 * 2**20
        ),
        name="retention",
    )(
        log_decay,
        inside,
        across,
        tokens.reshape(256, WIDTH),
        key_weight,
        queries.reshape(NB, 128, 128),
        values.reshape(NB, 128, 256),
        cotangent.reshape(2, 128, 4096),
    )
    return (
        gt.reshape(1, 256, WIDTH),
        gq.reshape(1, 4096, 1, 128),
        gv.reshape(1, 4096, 1, 256),
        dw.reshape(128, WIDTH),
    )


def solution(mesh):
    return jax.shard_map(
        body,
        mesh=mesh,
        in_specs=(
            P("dp", "sp", None),
            P("dp", None),
            P("dp", None, "sp", None),
            P("dp", None, "sp", None),
            P("dp", "sp", None),
            P(),
        ),
        out_specs=(
            P("dp", "sp", None),
            P("dp", None, "sp", None),
            P("dp", None, "sp", None),
            P("dp", None),
        ),
        check_vma=False,
    )
```

```python
import functools

import jax
import jax.numpy as jnp
import numpy as np
from jax import lax
from jax.experimental import pallas as pl
from jax.experimental.pallas import tpu as pltpu
from jax.sharding import PartitionSpec as P

MESH = pl.DeviceIdType.MESH
F32, BF16 = jnp.float32, jnp.bfloat16
BLOCK = 128
NB = 32
WIDTH = 2048
WA, WB = 640, 640
C1 = WA + WB
C2 = WIDTH - C1
ORDER = sorted(
    ((dy, dx) for dy in range(4) for dx in range(4) if dy or dx),
    key=lambda d: (-min(d[0], 4 - d[0]) - min(d[1], 4 - d[1]), -min(d[0], 4 - d[0])),
) + [(0, 0)]
FACTOR = BLOCK**-0.5


def tables():
    half = 64
    freq = 10000.0 ** (-np.arange(half, dtype=np.float64) / half)
    freq = np.concatenate([freq, freq])
    sign = np.where(np.arange(128) < half, -1.0, 1.0)
    ang_j = np.arange(128, dtype=np.float64)[:, None] * freq
    ang_n = 128.0 * np.arange(NB, dtype=np.float64)[:, None] * freq
    inside = np.stack([np.cos(ang_j), np.sin(ang_j), sign * np.cos(ang_j), sign * np.sin(ang_j)])
    across = np.stack([np.cos(ang_n), np.sin(ang_n)], axis=1)
    return inside.astype(np.float32), across.astype(np.float32)


def dot(a, b, ca, cb):
    return lax.dot_general(a, b, (((ca,), (cb,)), ((), ())), preferred_element_type=F32)


SCRATCH = dict(
    tok=((512, WIDTH), BF16),
    wall=((8, 128, WIDTH), BF16),
    vv=((NB, 128, 256), BF16),
    rq=((NB, 128, 128), BF16),
    dq=((NB, 128, 128), BF16),
    cosv=((NB, 128, 128), F32),
    sinv=((NB, 128, 128), F32),
    jtv=((4, 128, 128), F32),
    ntv=((NB, 2, 128), F32),
    within=((128, 128), F32),
    rise=((128, 128), F32),
    fall=((128, 128), F32),
    cot=((NB, 128, 256), BF16),
    mix=((NB, 128, 128), BF16),
    trl=((NB, 128, 256), F32),
    trb=((NB, 128, 256), BF16),
    entb=((NB, 128, 256), BF16),
    gko=((NB, 128, 128), BF16),
    gki=((4, 128, 1024), BF16),
    keyo=((8, 4, 128, 128), BF16),
    keyi=((NB, 128, 128), BF16),
    gts=((256, WIDTH), BF16),
    gtr=((256, WIDTH), BF16),
    dwz=((8, 128, C1), BF16),
    rza=((2, 4, 128, WA), BF16),
    rzb=((2, 4, 128, WB), BF16),
    dwx=((16, 8, 8, C2), BF16),
    rx=((16, 8, 8, C2), BF16),
    zx=((8, 8, C2), BF16),
    zr=((8, 8, C2), BF16),
    px=((16, 8, C1), BF16),
    pr=((16, 8, C1), BF16),
    fin=((16, 8, WIDTH), BF16),
)
SEMS = dict(
    loc=6, cot_s=1, cot_r=16, tok_s=1, tok_r=1, w_s=1, wp_r=7, wm_r=7, gk_s=2, gk_r=1, key_s=2, key_r=1,
    gt_s=1, gt_r=1, rz_s=1, rz_r=16, rx_s=1, rx_r=1, zx_s=1, zx_r=1, px_s=1, px_r=1, fin_s=1, fin_r=1,
)


def kernel(ld_ref, jt_ref, nt_ref, tok_ref, w_ref, q_ref, v_ref, cot_ref, gt_o, gq_o, gv_o, dw_o, *scratch):
    B = type("B", (), dict(zip([*SCRATCH, *SEMS], scratch, strict=True)))
    sp, dp = lax.axis_index("sp"), lax.axis_index("dp")
    y, x = lax.div(sp, 4), lax.rem(sp, 4)
    z, c = lax.div(dp, 2), lax.rem(dp, 2)
    head_core = lax.rem(x, 2)
    head_at = lax.div(sp, 2)

    def plane(t):
        if isinstance(t, int):
            dy, dx = ORDER[t]
        else:
            code = jnp.int32(0)
            for k, (a, b) in enumerate(ORDER[:15]):
                code = jnp.where(t == k, a * 4 + b, code)
            dy, dx = lax.div(code, 4), lax.rem(code, 4)
        to = lax.rem(y + dy, 4) * 4 + lax.rem(x + dx, 4)
        of = lax.rem(y + 4 - dy, 4) * 4 + lax.rem(x + 4 - dx, 4)
        return to, of

    def zat(dz):
        return lax.rem(z + 8 + dz, 8)

    def zdev(dz, core=c):
        return zat(dz) * 2 + core

    def remote(src, dst, ss, rs, dev):
        return pltpu.make_async_remote_copy(
            src_ref=src, dst_ref=dst, send_sem=ss, recv_sem=rs, device_id=dev, device_id_type=MESH
        )

    def arrived(ref, sem):
        pltpu.make_async_copy(ref, ref, sem).wait()

    def loop(lo, hi, f):
        def step(i, carry):
            f(i)
            return carry

        lax.fori_loop(lo, hi, step, 0)

    def lanes(i, width=128):
        return pl.ds(pl.multiple_of(i * width, width), width)

    bar = pltpu.get_barrier_semaphore()
    partner = (sp, zdev(0, 1 - c))

    def greet(k):
        for core in (c, 1 - c):
            pl.semaphore_signal(bar, inc=1, device_id=(lax.rem(sp + k, 16), zdev(0, core)), device_id_type=MESH)

    loop(1, 16, greet)
    pl.semaphore_signal(bar, inc=1, device_id=partner, device_id_type=MESH)
    loop(1, 8, lambda k: pl.semaphore_signal(bar, inc=1, device_id=(sp, zdev(k)), device_id_type=MESH))

    loads = [
        pltpu.make_async_copy(q_ref, B.rq, B.loc.at[0]),
        pltpu.make_async_copy(v_ref, B.vv, B.loc.at[1]),
        pltpu.make_async_copy(tok_ref, B.tok.at[pl.ds(c * 256, 256)], B.loc.at[2]),
        pltpu.make_async_copy(w_ref, B.wall.at[z], B.loc.at[3]),
        pltpu.make_async_copy(jt_ref, B.jtv, B.loc.at[4]),
        pltpu.make_async_copy(nt_ref, B.ntv, B.loc.at[5]),
        pltpu.make_async_copy(cot_ref.at[:, :, lanes(sp, 256)], B.cot.at[pl.ds(2 * sp, 2)], B.cot_r.at[sp]),
    ]
    for cp in loads:
        cp.start()
    pl.semaphore_wait(bar, 38)

    up, down = (sp, zdev(1)), (sp, zdev(-1))

    def w_copy(k, part, way):
        at = zat(-k if way == 0 else k)
        rows = pl.ds(64 * part, 64)
        sem = (B.wp_r if way == 0 else B.wm_r).at[2 * k + part if k < 3 else 6]
        src = w_ref.at[rows] if k == 0 else B.wall.at[at, rows]
        return remote(src, B.wall.at[at, rows], B.w_s.at[0], sem, up if way == 0 else down)

    def w_step(k, part):
        for way in (0, 1):
            if k == 4:
                arrived(B.wall.at[zat(4), pl.ds(64 * way, 64)], (B.wp_r, B.wm_r)[way].at[6])
                continue
            at = zat(-k if way == 0 else k)
            arrived(B.wall.at[at, pl.ds(64 * part, 64)], (B.wp_r, B.wm_r)[way].at[2 * (k - 1) + part])
            if k < 3 or part == way:
                w_copy(k, part, way).start()

    for part in range(2):
        for way in (0, 1):
            w_copy(0, part, way).start()

    def cot_copy(t):
        to, _ = plane(t)
        return remote(
            cot_ref.at[:, :, lanes(to, 256)], B.cot.at[pl.ds(2 * sp, 2)], B.cot_s.at[0], B.cot_r.at[sp], (to, dp)
        )

    for t in range(15):
        cot_copy(t).start()
    tok_copy = remote(tok_ref, B.tok.at[pl.ds(c * 256, 256)], B.tok_s.at[0], B.tok_r.at[0], partner)
    tok_copy.start()

    ld = ld_ref[sp]
    rows = lax.broadcasted_iota(jnp.int32, (128, 128), 0).astype(F32)
    cols = lax.broadcasted_iota(jnp.int32, (128, 128), 1).astype(F32)
    offset = rows - cols
    B.within[...] = jnp.where(offset >= 0, jnp.exp(jnp.maximum(offset, 0.0) * ld), 0.0)
    B.rise[...] = jnp.exp((rows + 1.0) * ld)
    B.fall[...] = jnp.exp((127.0 - rows) * ld)
    growth = jnp.exp(jnp.full((1, 256), 128.0, F32) * ld)
    loads[4].wait()
    loads[5].wait()
    loads[0].wait()

    def turn(n):
        cn, sn = B.ntv[n, 0:1, :], B.ntv[n, 1:2, :]
        cosine = cn * B.jtv[0] - sn * B.jtv[1]
        sine = sn * B.jtv[2] + cn * B.jtv[3]
        B.cosv[n] = cosine
        B.sinv[n] = sine
        u = B.rq[n].astype(F32)
        r = (u * cosine + pltpu.roll(u, 64, 1) * sine).astype(BF16)
        B.rq[n] = r
        B.dq[n] = (r.astype(F32) * B.rise[...]).astype(BF16)

    loop(0, NB, turn)

    def keys(hh):
        def part(i):
            k = dot(B.tok[pl.ds(pl.multiple_of(i * 256, 256), 256), :], B.wall[hh], 1, 1)
            B.keyo[hh, pl.ds(2 * i, 2)] = k.astype(BF16).reshape(2, 128, 128)

        loop(0, 2, part)

    def key_copy(hh, i, sem):
        return remote(
            B.keyo.at[hh, pl.ds(2 * i, 2)],
            B.keyi.at[pl.ds(2 * sp, 2)],
            B.key_s.at[sem],
            B.key_r.at[0],
            (2 * hh + c, zdev(0, i)),
        )

    own_head_here = head_core == c

    def key_send(hh):
        for i in range(2):
            special = jnp.logical_and(hh == head_at, c == i)

            @pl.when(jnp.logical_and(special, own_head_here))
            def _():
                pltpu.make_async_copy(
                    B.keyo.at[hh, pl.ds(2 * i, 2)], B.keyi.at[pl.ds(2 * sp, 2)], B.key_r.at[0]
                ).start()

            @pl.when(jnp.logical_and(special, jnp.logical_not(own_head_here)))
            def _():
                key_copy(hh, i, 1).start()

            @pl.when(jnp.logical_not(special))
            def _():
                key_copy(hh, i, 0).start()

    def cot_chunk(t):
        _, p = plane(t)
        arrived(B.cot.at[pl.ds(2 * p, 2)], B.cot_r.at[p])
        for b in range(2):
            n = 2 * p + b
            cb = B.cot[n]
            m = dot(cb, B.vv[n], 1, 1) * B.within[...]
            B.mix[n] = m.astype(BF16)
            B.trl[n] = dot(B.dq[n], cb, 0, 0)

    loads[2].wait()
    arrived(B.tok.at[pl.ds((1 - c) * 256, 256)], B.tok_r.at[0])
    loads[3].wait()
    loads[1].wait()
    loop(0, 1, lambda i: keys(zat(0)))
    w_step(1, 0)
    loop(0, 3, cot_chunk)
    w_step(1, 1)
    loop(0, 2, lambda i: keys(zat(2 * i - 1)))
    loop(3, 7, cot_chunk)
    w_step(2, 0)
    loop(7, 12, cot_chunk)
    w_step(2, 1)
    loop(12, 16, cot_chunk)
    def scan(i, carry):
        n = NB - 1 - i
        B.trb[n] = carry.astype(BF16)
        return B.trl[n] + growth * carry

    lax.fori_loop(0, NB, scan, jnp.zeros((128, 256), F32))

    def gk_copy(t, sem=0):
        to, _ = plane(t)
        return remote(
            B.gko.at[pl.ds(2 * to, 2)],
            B.gki.at[pl.ds(2 * c, 2), :, lanes(head_at)],
            B.gk_s.at[sem],
            B.gk_r.at[0],
            (to, zdev(0, head_core)),
        )

    def gk_chunk(t):
        p, _ = plane(t)
        for b in range(2):
            n = 2 * p + b
            g = dot(B.mix[n], B.rq[n], 0, 0) + B.fall[...] * dot(B.vv[n], B.trb[n], 1, 1)
            g = g * B.cosv[n] - pltpu.roll(g, 64, 1) * B.sinv[n]
            B.gko[n] = (g * FACTOR).astype(BF16)

        @pl.when(t < 15)
        def _():
            gk_copy(t).start()

    loop(0, 8, gk_chunk)
    w_step(3, 0)
    loop(8, 16, gk_chunk)

    @pl.when(own_head_here)
    def _():
        pltpu.make_async_copy(
            B.gko.at[pl.ds(2 * sp, 2)], B.gki.at[pl.ds(2 * c, 2), :, lanes(head_at)], B.gk_r.at[0]
        ).start()

    @pl.when(jnp.logical_not(own_head_here))
    def _():
        gk_copy(15, 1).start()

    w_step(3, 1)
    loop(0, 4, lambda i: keys(zat(i - 3 + lax.div(i, 2) * 3)))

    arrived(B.gki, B.gk_r.at[0])
    def ring_refs(way, half, k):
        lo, width = (0, WA) if half == 0 else (WA, WB)
        return pl.ds(lo, width), (B.rza if half == 0 else B.rzb).at[way, k - 1], B.rz_r.at[(way * 2 + half) * 4 + k - 1]

    def ring_send(way, half, k):
        at, dst, sem = ring_refs(way, half, k)
        d = zat(k if way == 0 else -k)
        remote(B.dwz.at[d, :, at], dst, B.rz_s.at[0], sem, up if way == 0 else down).start()

    def ring_take(way, half, k):
        at, got, sem = ring_refs(way, half, k)
        arrived(got, sem)
        if k == 1:
            return
        d = zat(k - 1 if way == 0 else 1 - k)

        def add(i):
            r = pl.ds(pl.multiple_of(i * 16, 16), 16)
            B.dwz[d, r, at] = (B.dwz[d, r, at].astype(F32) + got[r, :].astype(F32)).astype(BF16)

        loop(0, 8, add)
        ring_send(way, half, k - 1)

    def dw_part(hh, lo, hi):
        a = B.gki[:, :, lanes(hh)].reshape(512, 128)
        for at in range(lo, hi, 256):
            g = dot(a, B.tok[:, at : at + 256], 0, 0)
            if at < C1:
                B.dwz[hh, :, at : at + 256] = g.astype(BF16)
            else:
                B.dwx[:, hh, :, at - C1 : at - C1 + 256] = g.reshape(16, 8, 256).astype(BF16)

    def dwz_head(t):
        r, i = lax.rem(t, 2), lax.div(t, 2)
        dw_part(zat(r * (3 - i) + (1 - r) * (4 + i)), 0, C1)

        @pl.when(t == 0)
        def _():
            ring_send(0, 0, 4)
            ring_send(1, 1, 4)

        @pl.when(t == 1)
        def _():
            ring_send(0, 1, 3)

        @pl.when(t == 2)
        def _():
            ring_send(1, 0, 3)

    loop(0, 3, dwz_head)
    loop(0, 8, lambda hh: dw_part(hh, C1, WIDTH))
    for t in range(15):
        to, _ = plane(t)
        remote(B.dwx.at[to], B.rx.at[sp], B.rx_s.at[0], B.rx_r.at[0], (to, dp)).start()
    def later(i):
        key_send(zat(lax.rem(sp + i, 7) - 3))

    loop(0, 7, later)
    loop(3, 8, dwz_head)
    ring_take(0, 0, 4)
    ring_take(1, 1, 4)
    w_step(4, 0)
    loop(0, 1, lambda i: keys(zat(4)))
    key_send(zat(4))
    ring_take(0, 1, 3)
    ring_take(1, 0, 3)

    def gt_tile(first):
        def tile(i):
            j = (1 - c) if first else c
            a = jnp.concatenate([B.gki[2 * j], B.gki[2 * j + 1]], axis=0)
            g = dot(a, B.wall[:, :, lanes(i, 256)].reshape(1024, 256), 1, 0)
            if first:
                B.gts[:, lanes(i, 256)] = g.astype(BF16)
            else:
                gt_o[:, lanes(i, 256)] = (g + B.gtr[:, lanes(i, 256)].astype(F32)).astype(BF16)

        return tile

    loop(0, 8, gt_tile(True))
    gt_copy = remote(B.gts, B.gtr, B.gt_s.at[0], B.gt_r.at[0], partner)
    gt_copy.start()
    ring_take(0, 0, 3)
    ring_take(1, 1, 3)
    arrived(B.gtr, B.gt_r.at[0])
    loop(0, 8, gt_tile(False))
    ring_take(0, 1, 2)
    ring_take(1, 0, 2)

    def back_a(i):
        for b in range(4):
            n = 4 * i + b
            u = B.keyi[n].astype(F32)
            rk = ((u * B.cosv[n] + pltpu.roll(u, 64, 1) * B.sinv[n]) * FACTOR).astype(BF16)
            B.keyi[n] = rk
            B.dq[n] = (dot(B.rq[n], rk, 1, 1) * B.within[...]).astype(BF16)
            dk = (rk.astype(F32) * B.fall[...]).astype(BF16)
            B.trl[n] = dot(dk, B.vv[n], 0, 0)

    def scan_up(n, carry):
        B.entb[n] = carry.astype(BF16)
        return B.trl[n] + growth * carry

    def back_c(i):
        for b in range(4):
            n = 4 * i + b
            rk, cb, f = B.keyi[n], B.cot[n], B.fall[...]
            g = dot(B.mix[n], rk, 1, 0) + B.rise[...] * dot(cb, B.entb[n], 1, 1)
            gq_o[n] = (g * B.cosv[n] - pltpu.roll(g, 64, 1) * B.sinv[n]).astype(BF16)
            near, far = dot(B.dq[n], cb, 0, 0), dot(rk, B.trb[n], 1, 0)
            for h in range(2):
                at = slice(128 * h, 128 * h + 128)
                gv_o[n, :, at] = (near[:, at] + f * far[:, at]).astype(BF16)

    ring_take(0, 0, 2)
    ring_take(1, 1, 2)
    ring_take(0, 1, 1)
    ring_take(1, 0, 1)
    arrived(B.rx.at[0:15], B.rx_r.at[0])
    B.rx[sp] = B.dwx[sp]

    def plane_sum(d):
        total = B.rx[0, d].astype(F32)
        for p in range(1, 16):
            total += B.rx[p, d].astype(F32)
        B.zx[d] = total.astype(BF16)

    loop(0, 8, plane_sum)
    for k in range(1, 8):
        d = zat(k)
        remote(B.zx.at[d], B.zr.at[z], B.zx_s.at[0], B.zx_r.at[0], (sp, zdev(k))).start()
    ring_take(0, 0, 1)
    ring_take(1, 1, 1)

    def owned(i):
        r = pl.ds(pl.multiple_of(i * 16, 16), 16)
        for got, lo, width in ((B.rza, 0, WA), (B.rzb, WA, WB)):
            v = B.dwz[z, r, lo : lo + width].astype(F32)
            v += got[0, 0, r, :].astype(F32) + got[1, 0, r, :].astype(F32)
            B.px[pl.ds(2 * i, 2), :, lo : lo + width] = v.reshape(2, 8, width).astype(BF16)

    loop(0, 8, owned)
    for t in range(15):
        to, _ = plane(t)
        remote(B.px.at[to], B.pr.at[sp], B.px_s.at[0], B.px_r.at[0], (to, dp)).start()

    arrived(B.keyi, B.key_r.at[0])
    loop(0, 8, back_a)
    lax.fori_loop(0, NB, scan_up, jnp.zeros((128, 256), F32))

    arrived(B.zr.at[0:7], B.zx_r.at[0])
    B.zr[z] = B.zx[z]
    total = B.zr[0].astype(F32)
    for k in range(1, 8):
        total += B.zr[k].astype(F32)
    B.fin[sp, :, C1:WIDTH] = total.astype(BF16)
    B.pr[sp] = B.px[sp]
    arrived(B.pr.at[0:15], B.px_r.at[0])
    total = B.pr[0].astype(F32)
    for p in range(1, 16):
        total += B.pr[p].astype(F32)
    B.fin[sp, :, 0:C1] = total.astype(BF16)
    for t in range(15):
        to, _ = plane(t)
        remote(B.fin.at[sp], B.fin.at[sp], B.fin_s.at[0], B.fin_r.at[0], (to, dp)).start()
    loop(0, 8, back_c)
    arrived(B.fin.at[0:15], B.fin_r.at[0])

    def widen(j):
        dw_o[j] = B.fin[j].astype(F32)

    loop(0, 16, widen)

    arrived(B.cot.at[0:30], B.cot_s.at[0])
    arrived(B.wall.at[0:7], B.w_s.at[0])
    tok_copy.wait_send()
    gt_copy.wait_send()
    arrived(B.gko.at[0:30], B.gk_s.at[0])
    arrived(B.keyi.at[0:30], B.key_s.at[0])

    @pl.when(jnp.logical_not(own_head_here))
    def _():
        arrived(B.gko.at[0:2], B.gk_s.at[1])
        arrived(B.keyi.at[0:2], B.key_s.at[1])

    arrived(B.dwz.at[0:7], B.rz_s.at[0])
    arrived(B.dwx.at[0:15], B.rx_s.at[0])
    arrived(B.px.at[0:15], B.px_s.at[0])
    arrived(B.zx.at[0:7], B.zx_s.at[0])
    arrived(B.fin.at[0:15], B.fin_s.at[0])


def body(tokens, key_weight, queries, values, cotangent, log_decay):
    inside, across = tables()
    hbm, vmem = pl.BlockSpec(memory_space=pltpu.HBM), pl.BlockSpec(memory_space=pltpu.VMEM)
    shapes = [
        jax.ShapeDtypeStruct((256, WIDTH), BF16),
        jax.ShapeDtypeStruct((NB, 128, 128), BF16),
        jax.ShapeDtypeStruct((NB, 128, 256), BF16),
        jax.ShapeDtypeStruct((16, 8, WIDTH), F32),
    ]
    gt, gq, gv, dw = pl.pallas_call(
        kernel,
        out_shape=shapes,
        in_specs=[pl.BlockSpec(memory_space=pltpu.SMEM)] + [hbm] * 7,
        out_specs=[vmem] * 4,
        scratch_shapes=[pltpu.VMEM(shape, kind) for shape, kind in SCRATCH.values()]
        + [pltpu.SemaphoreType.DMA((n,)) for n in SEMS.values()],
        compiler_params=pltpu.CompilerParams(
            collective_id=0, has_side_effects=True, vmem_limit_bytes=48 * 2**20
        ),
        name="retention",
    )(
        log_decay,
        *(
            pltpu.with_memory_space_constraint(a, pltpu.HBM)
            for a in (
                jnp.asarray(inside),
                jnp.asarray(across),
                tokens.reshape(256, WIDTH),
                key_weight,
                queries.reshape(NB, 128, 128),
                values.reshape(NB, 128, 256),
                cotangent.reshape(2, 128, 4096),
            )
        ),
    )
    return (
        gt.reshape(1, 256, WIDTH),
        gq.reshape(1, 4096, 1, 128),
        gv.reshape(1, 4096, 1, 256),
        dw.reshape(128, WIDTH),
    )


def solution(mesh):
    return jax.shard_map(
        body,
        mesh=mesh,
        in_specs=(
            P("dp", "sp", None),
            P("dp", None),
            P("dp", None, "sp", None),
            P("dp", None, "sp", None),
            P("dp", "sp", None),
            P(),
        ),
        out_specs=(
            P("dp", "sp", None),
            P("dp", None, "sp", None),
            P("dp", None, "sp", None),
            P("dp", None),
        ),
        check_vma=False,
    )
```

```python
import functools

import jax
import jax.numpy as jnp
import numpy as np
from jax import lax
from jax.experimental import pallas as pl
from jax.experimental.pallas import tpu as pltpu
from jax.sharding import PartitionSpec as P

MESH = pl.DeviceIdType.MESH
F32, BF16 = jnp.float32, jnp.bfloat16
BLOCK = 128
NB = 32
WIDTH = 2048
CHAINS, CW = 3, 256
C1 = CHAINS * CW
C2 = WIDTH - C1
H2 = C2 // 2
ORDER = (
    (1, 1), (3, 3), (3, 1), (1, 3), (2, 1), (2, 3), (1, 2), (3, 2), (2, 2), (1, 0), (3, 0), (0, 2), (2, 0), (0, 1), (0, 3),
    (0, 0),
)
FACTOR = BLOCK**-0.5


def tables():
    half = 64
    freq = 10000.0 ** (-np.arange(half, dtype=np.float64) / half)
    freq = np.concatenate([freq, freq])
    sign = np.where(np.arange(128) < half, -1.0, 1.0)
    ang_j = np.arange(128, dtype=np.float64)[:, None] * freq
    ang_n = 128.0 * np.arange(NB, dtype=np.float64)[:, None] * freq
    inside = np.stack([np.cos(ang_j), np.sin(ang_j), sign * np.cos(ang_j), sign * np.sin(ang_j)])
    across = np.stack([np.cos(ang_n), np.sin(ang_n)], axis=1)
    return inside.astype(np.float32), across.astype(np.float32)


def dot(a, b, ca, cb):
    return lax.dot_general(a, b, (((ca,), (cb,)), ((), ())), preferred_element_type=F32)


QUARTERS = (
    (((2, 0), (2, 1)), ((0, 2), (0, 3))),
    (((1, 2), (1, 3)), ((3, 0), (3, 1))),
    (((1, 0), (1, 1)), ((3, 2), (3, 3))),
    (((0, 0), (0, 1)), ((2, 2), (2, 3))),
)

SCRATCH = dict(
    tok=((512, WIDTH), BF16),
    wall=((8, 128, WIDTH), BF16),
    vv=((NB, 128, 256), BF16),
    rq=((NB, 128, 128), BF16),
    dq=((NB, 128, 128), BF16),
    cosv=((NB, 128, 128), F32),
    sinv=((NB, 128, 128), F32),
    jtv=((4, 128, 128), F32),
    ntv=((NB, 2, 128), F32),
    within=((128, 128), F32),
    rise=((128, 128), F32),
    fall=((128, 128), F32),
    cot=((NB, 128, 256), BF16),
    mix=((NB, 128, 128), BF16),
    trl=((NB, 128, 256), F32),
    trb=((NB, 128, 256), BF16),
    entb=((NB, 128, 256), BF16),
    gko=((NB, 128, 128), BF16),
    gki=((4, 128, 1024), BF16),
    gkt=((1024, 512), BF16),
    keyo=((8, 4, 128, 128), BF16),
    keyi=((NB, 128, 128), BF16),
    gts=((256, WIDTH), BF16),
    gtr=((256, WIDTH), BF16),
    dwz=((8, 128, C1), BF16),
    rz=((CHAINS, 2, 4, 128, CW), BF16),
    dwx=((2, 4, 4, 8, 8, H2), BF16),
    f1=((2, 2, 2, 8, 8, H2), BF16),
    r1=((2, 2, 4, 8, 8, H2), BF16),
    s1=((2, 4, 8, 8, H2), BF16),
    r2=((2, 4, 8, 8, H2), BF16),
    zx=((8, 8, C2), BF16),
    zr=((8, 8, C2), BF16),
    px=((16, 8, C1), BF16),
    pr=((16, 8, C1), BF16),
    fin=((16, 8, WIDTH), BF16),
)
SEMS = dict(
    loc=7, cot_s=1, cot_r=16, tok_s=1, tok_r=1, w_s=1, wp_r=7, wm_r=7, gk_s=2, gk_r=1, key_s=2, key_r=1,
    gt_s=1, gt_r=1, rz_s=1, rz_r=8 * CHAINS, f1_r=4, r1_s=1, r1_r=1, r2_s=1, r2_r=1, zx_s=1, zx_r=1, px_s=1, px_r=1, fin_s=1, finx_r=1, finz_r=1,
)


def kernel(ld_ref, jt_ref, nt_ref, tok_ref, w_ref, q_ref, v_ref, cot_ref, gt_o, gq_o, gv_o, dw_o, *scratch):
    B = type("B", (), dict(zip([*SCRATCH, *SEMS, "lds"], scratch, strict=True)))
    sp, dp = lax.axis_index("sp"), lax.axis_index("dp")
    y, x = lax.div(sp, 4), lax.rem(sp, 4)
    z, c = lax.div(dp, 2), lax.rem(dp, 2)
    head_core = lax.rem(x, 2)
    head_at = lax.div(sp, 2)

    def plane(t):
        if isinstance(t, int):
            dy, dx = ORDER[t]
        else:
            code = jnp.int32(0)
            for k, (a, b) in enumerate(ORDER[:15]):
                code = jnp.where(t == k, a * 4 + b, code)
            dy, dx = lax.div(code, 4), lax.rem(code, 4)
        to = lax.rem(y + dy, 4) * 4 + lax.rem(x + dx, 4)
        of = lax.rem(y + 4 - dy, 4) * 4 + lax.rem(x + 4 - dx, 4)
        return to, of

    def zat(dz):
        return lax.rem(z + 8 + dz, 8)

    def zdev(dz, core=c):
        return zat(dz) * 2 + core

    def remote(src, dst, ss, rs, dev):
        return pltpu.make_async_remote_copy(
            src_ref=src, dst_ref=dst, send_sem=ss, recv_sem=rs, device_id=dev, device_id_type=MESH
        )

    def arrived(ref, sem):
        pltpu.make_async_copy(ref, ref, sem).wait()

    def loop(lo, hi, f):
        def step(i, carry):
            f(i)
            return carry

        lax.fori_loop(lo, hi, step, 0)

    def lanes(i, width=128):
        return pl.ds(pl.multiple_of(i * width, width), width)

    bar = pltpu.get_barrier_semaphore()
    partner = (sp, zdev(0, 1 - c))

    def greet(k):
        for core in (c, 1 - c):
            pl.semaphore_signal(bar, inc=1, device_id=(lax.rem(sp + k, 16), zdev(0, core)), device_id_type=MESH)

    loop(1, 16, greet)
    pl.semaphore_signal(bar, inc=1, device_id=partner, device_id_type=MESH)
    loop(1, 8, lambda k: pl.semaphore_signal(bar, inc=1, device_id=(sp, zdev(k)), device_id_type=MESH))

    loads = [
        pltpu.make_async_copy(ld_ref, B.lds, B.loc.at[6]),
        pltpu.make_async_copy(q_ref, B.rq, B.loc.at[0]),
        pltpu.make_async_copy(v_ref, B.vv, B.loc.at[1]),
        pltpu.make_async_copy(tok_ref, B.tok.at[pl.ds(c * 256, 256)], B.loc.at[2]),
        pltpu.make_async_copy(w_ref, B.wall.at[z], B.loc.at[3]),
        pltpu.make_async_copy(jt_ref, B.jtv, B.loc.at[4]),
        pltpu.make_async_copy(nt_ref, B.ntv, B.loc.at[5]),
        pltpu.make_async_copy(cot_ref.at[:, :, lanes(sp, 256)], B.cot.at[pl.ds(2 * sp, 2)], B.cot_r.at[sp]),
    ]
    for cp in loads:
        cp.start()
    pl.semaphore_wait(bar, 38)

    up, down = (sp, zdev(1)), (sp, zdev(-1))

    def w_copy(k, part, way):
        at = zat(-k if way == 0 else k)
        rows = pl.ds(64 * part, 64)
        sem = (B.wp_r if way == 0 else B.wm_r).at[2 * k + part if k < 3 else 6]
        src = w_ref.at[rows] if k == 0 else B.wall.at[at, rows]
        return remote(src, B.wall.at[at, rows], B.w_s.at[0], sem, up if way == 0 else down)

    def w_step(k, part):
        for way in (0, 1):
            if k == 4:
                arrived(B.wall.at[zat(4), pl.ds(64 * way, 64)], (B.wp_r, B.wm_r)[way].at[6])
                continue
            at = zat(-k if way == 0 else k)
            arrived(B.wall.at[at, pl.ds(64 * part, 64)], (B.wp_r, B.wm_r)[way].at[2 * (k - 1) + part])
            if k < 3 or part == way:
                w_copy(k, part, way).start()

    for part in range(2):
        for way in (0, 1):
            w_copy(0, part, way).start()

    def cot_copy(t):
        to, _ = plane(t)
        return remote(
            cot_ref.at[:, :, lanes(to, 256)], B.cot.at[pl.ds(2 * sp, 2)], B.cot_s.at[0], B.cot_r.at[sp], (to, dp)
        )

    for t in range(15):
        cot_copy(t).start()
    tok_copy = remote(tok_ref, B.tok.at[pl.ds(c * 256, 256)], B.tok_s.at[0], B.tok_r.at[0], partner)
    tok_copy.start()

    loads[0].wait()
    ld = B.lds[sp]
    rows = lax.broadcasted_iota(jnp.int32, (128, 128), 0).astype(F32)
    cols = lax.broadcasted_iota(jnp.int32, (128, 128), 1).astype(F32)
    offset = rows - cols
    B.within[...] = jnp.where(offset >= 0, jnp.exp(jnp.maximum(offset, 0.0) * ld), 0.0)
    B.rise[...] = jnp.exp((rows + 1.0) * ld)
    B.fall[...] = jnp.exp((127.0 - rows) * ld)
    growth = jnp.exp(jnp.full((1, 256), 128.0, F32) * ld)
    loads[5].wait()
    loads[6].wait()
    loads[1].wait()

    def turn(n):
        cn, sn = B.ntv[n, 0:1, :], B.ntv[n, 1:2, :]
        cosine = cn * B.jtv[0] - sn * B.jtv[1]
        sine = sn * B.jtv[2] + cn * B.jtv[3]
        B.cosv[n] = cosine
        B.sinv[n] = sine
        u = B.rq[n].astype(F32)
        r = (u * cosine + pltpu.roll(u, 64, 1) * sine).astype(BF16)
        B.rq[n] = r
        B.dq[n] = (r.astype(F32) * B.rise[...]).astype(BF16)

    loop(0, NB, turn)

    def keys(hh):
        def part(i):
            k = dot(B.tok[pl.ds(pl.multiple_of(i * 256, 256), 256), :], B.wall[hh], 1, 1)
            B.keyo[hh, pl.ds(2 * i, 2)] = k.astype(BF16).reshape(2, 128, 128)

        loop(0, 2, part)

    def key_copy(hh, i, sem):
        return remote(
            B.keyo.at[hh, pl.ds(2 * i, 2)],
            B.keyi.at[pl.ds(2 * sp, 2)],
            B.key_s.at[sem],
            B.key_r.at[0],
            (2 * hh + c, zdev(0, i)),
        )

    own_head_here = head_core == c

    def key_send(hh):
        for i in range(2):
            special = jnp.logical_and(hh == head_at, c == i)

            @pl.when(jnp.logical_and(special, own_head_here))
            def _():
                pltpu.make_async_copy(
                    B.keyo.at[hh, pl.ds(2 * i, 2)], B.keyi.at[pl.ds(2 * sp, 2)], B.key_r.at[0]
                ).start()

            @pl.when(jnp.logical_and(special, jnp.logical_not(own_head_here)))
            def _():
                key_copy(hh, i, 1).start()

            @pl.when(jnp.logical_not(special))
            def _():
                key_copy(hh, i, 0).start()

    def cot_chunk(t):
        _, p = plane(t)
        arrived(B.cot.at[pl.ds(2 * p, 2)], B.cot_r.at[p])
        for b in range(2):
            n = 2 * p + b
            cb = B.cot[n]
            m = dot(cb, B.vv[n], 1, 1) * B.within[...]
            B.mix[n] = m.astype(BF16)
            B.trl[n] = dot(B.dq[n], cb, 0, 0)

    def take_tokens():
        loads[3].wait()
        arrived(B.tok.at[pl.ds((1 - c) * 256, 256)], B.tok_r.at[0])
        loads[4].wait()
        loads[2].wait()

    def keys_of(first, step, count):
        loop(0, count, lambda i: keys(zat(first + step * i)))

    def mixing(lo, hi):
        loop(lo, hi, cot_chunk)

    def scan(i, carry):
        n = NB - 1 - i
        B.trb[n] = carry.astype(BF16)
        return B.trl[n] + growth * carry

    def trails():
        lax.fori_loop(0, NB, scan, jnp.zeros((128, 256), F32))

    def gk_copy(t, sem=0):
        to, _ = plane(t)
        return remote(
            B.gko.at[pl.ds(2 * to, 2)],
            B.gki.at[pl.ds(2 * c, 2), :, lanes(head_at)],
            B.gk_s.at[sem],
            B.gk_r.at[0],
            (to, zdev(0, head_core)),
        )

    def gk_chunk(t):
        p, _ = plane(t)
        for b in range(2):
            n = 2 * p + b
            g = dot(B.mix[n], B.rq[n], 0, 0) + B.fall[...] * dot(B.vv[n], B.trb[n], 1, 1)
            g = g * B.cosv[n] - pltpu.roll(g, 64, 1) * B.sinv[n]
            B.gko[n] = (g * FACTOR).astype(BF16)

        @pl.when(t < 15)
        def _():
            gk_copy(t).start()

    def key_grads(lo, hi):
        loop(lo, hi, gk_chunk)
        if hi < 16:
            return

        @pl.when(own_head_here)
        def _():
            pltpu.make_async_copy(
                B.gko.at[pl.ds(2 * sp, 2)], B.gki.at[pl.ds(2 * c, 2), :, lanes(head_at)], B.gk_r.at[0]
            ).start()

        @pl.when(jnp.logical_not(own_head_here))
        def _():
            gk_copy(15, 1).start()

    def take_key_grads():
        arrived(B.gki, B.gk_r.at[0])
        for i in range(4):
            B.gkt[:, 128 * i : 128 * i + 128] = B.gki[i].T

    def send_keys(part):
        even = lax.rem(x + c, 2) == 0
        for (y0, x0), (y1, x1) in QUARTERS[part]:
            to = lax.rem(y + jnp.where(even, y0, y1), 4) * 4 + lax.rem(x + jnp.where(even, x0, x1), 4)
            key_send(lax.div(to, 2))

    def ring_refs(chain, way, k):
        at = pl.ds(chain * CW, CW)
        return at, B.rz.at[chain, way, k - 1], B.rz_r.at[(chain * 2 + way) * 4 + k - 1]

    def ring_send(chain, way, k):
        at, dst, sem = ring_refs(chain, way, k)
        d = zat(k if way == 0 else -k)
        remote(B.dwz.at[d, :, at], dst, B.rz_s.at[0], sem, up if way == 0 else down).start()

    def ring_take(chain, way, k):
        at, got, sem = ring_refs(chain, way, k)
        arrived(got, sem)
        if k == 1:
            return
        d = zat(k - 1 if way == 0 else 1 - k)

        def add(i):
            r = pl.ds(pl.multiple_of(i * 32, 32), 32)
            B.dwz[d, r, at] = (B.dwz[d, r, at].astype(F32) + got[r, :].astype(F32)).astype(BF16)

        loop(0, 4, add)
        ring_send(chain, way, k - 1)

    def take(chain, k):
        ring_take(chain, chain % 2, k)
        if k > 1:
            ring_take(chain, 1 - chain % 2, k - 1)

    def weight_ring(lo, hi):
        def tile(i):
            g = dot(B.gkt[...], B.tok[:, lanes(i, CW)], 1, 0)
            B.dwz[:, :, lanes(i, CW)] = g.astype(BF16).reshape(8, 128, CW)

        loop(lo, hi, tile)
        for chain in range(lo, hi):
            ring_send(chain, chain % 2, 4)
            ring_send(chain, 1 - chain % 2, 3)

    def line(way, step):
        if way == 0:
            at = lax.rem(x + step, 4)
            return at, x, (y * 4 + at, dp)
        at = lax.rem(y + step, 4)
        return at, y, (at * 4 + x, dp)

    def weight_plane(way):
        def tile(at, width):
            g = dot(B.gkt[...], B.tok[:, pl.ds(C1 + way * H2 + at, width)], 1, 0)
            g = g.astype(BF16).reshape(8, 4, 4, 8, width)
            for yy in range(4):
                for xx in range(4):
                    a1, a2 = (xx, yy) if way == 0 else (yy, xx)
                    B.dwx[way, a1, a2, :, :, pl.ds(at, width)] = g[:, yy, xx]

        if H2 % 256 == 0:
            loop(0, H2 // 256, lambda i: tile(pl.multiple_of(i * 256, 256), 256))
        else:
            for at in range(0, H2, 256):
                tile(at, min(256, H2 - at))
        for step in (1, 3):
            near, _, dev = line(way, step)
            far, _, _ = line(way, 2)
            side = 0 if step == 1 else 1
            through, own = pl.ds(2 * side, 2), pl.ds(2 - 2 * side, 2)
            remote(B.dwx.at[way, far, through], B.f1.at[way, side], B.r1_s.at[0], B.f1_r.at[2 * way + side], dev).start()
            remote(B.dwx.at[way, near, own], B.r1.at[way, side, own], B.r1_s.at[0], B.r1_r.at[0], dev).start()

    def line_pass(way):
        for step in (1, 3):
            near, _, dev = line(way, step)
            side = 0 if step == 1 else 1
            arrived(B.f1.at[way, side], B.f1_r.at[2 * way + side])

            def add(i):
                j, hh = lax.div(i, 4), lax.rem(i, 4) * 2
                have = B.dwx[way, near, 2 * side + j, pl.ds(hh, 2)].astype(F32)
                B.dwx[way, near, 2 * side + j, pl.ds(hh, 2)] = (have + B.f1[way, side, j, pl.ds(hh, 2)].astype(F32)).astype(BF16)

            loop(0, 8, add)
            through = pl.ds(2 * side, 2)
            remote(
                B.dwx.at[way, near, through], B.r1.at[way, side, through], B.r1_s.at[0], B.r1_r.at[0], dev
            ).start()

    def line_sums():
        arrived(B.r1, B.r1_r.at[0])
        for way, me in ((0, x), (1, y)):

            def add(i):
                j, hh = lax.div(i, 4), lax.rem(i, 4) * 2
                total = B.dwx[way, me, j, pl.ds(hh, 2)].astype(F32)
                for side in range(2):
                    total += B.r1[way, side, j, pl.ds(hh, 2)].astype(F32)
                B.s1[way, j, pl.ds(hh, 2)] = total.astype(BF16)

            loop(0, 16, add)
        for step in (2, 1, 3):
            for way in (0, 1):
                at, me, dev = line(1 - way, step)
                remote(B.s1.at[way, at], B.r2.at[way, me], B.r2_s.at[0], B.r2_r.at[0], dev).start()

    def plane_sums():
        arrived(B.r2.at[:, 0:3], B.r2_r.at[0])
        for way, me in ((0, y), (1, x)):
            B.r2[way, me] = B.s1[way, me]
            for hh in range(8):
                total = B.r2[way, 0, hh].astype(F32)
                for p in range(1, 4):
                    total += B.r2[way, p, hh].astype(F32)
                B.zx[hh, :, way * H2 : way * H2 + H2] = total.astype(BF16)
        for k in range(1, 8):
            d = zat(k)
            remote(B.zx.at[d], B.zr.at[z], B.zx_s.at[0], B.zx_r.at[0], (sp, zdev(k))).start()

    def own_rows(i):
        r = pl.ds(pl.multiple_of(i * 16, 16), 16)
        for chain in range(CHAINS):
            at = slice(chain * CW, chain * CW + CW)
            v = B.dwz[z, r, at].astype(F32) + B.rz[chain, 0, 0, r, :].astype(F32) + B.rz[chain, 1, 0, r, :].astype(F32)
            B.px[pl.ds(2 * i, 2), :, at] = v.reshape(2, 8, CW).astype(BF16)

    def column_sums():
        loop(0, 8, own_rows)
        for t in range(15):
            to, _ = plane(t)
            remote(B.px.at[to], B.pr.at[sp], B.px_s.at[0], B.px_r.at[0], (to, dp)).start()

    def total_of(ref, count):
        total = ref[0].astype(F32)
        for p in range(1, count):
            total += ref[p].astype(F32)
        return total.astype(BF16)

    def fin_send(lo, hi, sem):
        for t in range(15):
            to, _ = plane(t)
            ref = B.fin.at[sp, :, pl.ds(lo, hi - lo)]
            remote(ref, ref, B.fin_s.at[0], sem, (to, dp)).start()

    def finish_plane_part():
        arrived(B.zr.at[0:7], B.zx_r.at[0])
        B.zr[z] = B.zx[z]
        B.fin[sp, :, C1:WIDTH] = total_of(B.zr, 8)
        fin_send(C1, WIDTH, B.finx_r.at[0])

    def finish_ring_part():
        B.pr[sp] = B.px[sp]
        arrived(B.pr.at[0:15], B.px_r.at[0])
        B.fin[sp, :, 0:C1] = total_of(B.pr, 16)
        fin_send(0, C1, B.finz_r.at[0])

    def widen(j):
        dw_o[j] = B.fin[j].astype(F32)

    def weight_out():
        arrived(B.fin.at[0:15, :, C1:WIDTH], B.finx_r.at[0])
        arrived(B.fin.at[0:15, :, 0:C1], B.finz_r.at[0])
        loop(0, 16, widen)

    def gt_tile(first):
        def tile(i):
            j = (1 - c) if first else c
            a = jnp.concatenate([B.gki[2 * j], B.gki[2 * j + 1]], axis=0)
            g = dot(a, B.wall[:, :, lanes(i, 256)].reshape(1024, 256), 1, 0)
            if first:
                B.gts[:, lanes(i, 256)] = g.astype(BF16)
            else:
                gt_o[:, lanes(i, 256)] = (g + B.gtr[:, lanes(i, 256)].astype(F32)).astype(BF16)

        return tile

    gt_copy = remote(B.gts, B.gtr, B.gt_s.at[0], B.gt_r.at[0], partner)

    def token_grads_partner(lo, hi):
        loop(lo, hi, gt_tile(True))
        if hi == 8:
            gt_copy.start()

    def token_grads(lo, hi):
        if lo == 0:
            arrived(B.gtr, B.gt_r.at[0])
        loop(lo, hi, gt_tile(False))

    def back_a(i):
        for b in range(4):
            n = 4 * i + b
            u = B.keyi[n].astype(F32)
            rk = ((u * B.cosv[n] + pltpu.roll(u, 64, 1) * B.sinv[n]) * FACTOR).astype(BF16)
            B.keyi[n] = rk
            B.dq[n] = (dot(B.rq[n], rk, 1, 1) * B.within[...]).astype(BF16)
            dk = (rk.astype(F32) * B.fall[...]).astype(BF16)
            B.trl[n] = dot(dk, B.vv[n], 0, 0)

    def scan_up(n, carry):
        B.entb[n] = carry.astype(BF16)
        return B.trl[n] + growth * carry

    def back_c(i):
        for b in range(4):
            n = 4 * i + b
            rk, cb, f = B.keyi[n], B.cot[n], B.fall[...]
            g = dot(B.mix[n], rk, 1, 0) + B.rise[...] * dot(cb, B.entb[n], 1, 1)
            gq_o[n] = (g * B.cosv[n] - pltpu.roll(g, 64, 1) * B.sinv[n]).astype(BF16)
            near, far = dot(B.dq[n], cb, 0, 0), dot(rk, B.trb[n], 1, 0)
            for h in range(2):
                at = slice(128 * h, 128 * h + 128)
                gv_o[n, :, at] = (near[:, at] + f * far[:, at]).astype(BF16)

    def take_keys():
        arrived(B.keyi, B.key_r.at[0])

    def scores(lo, hi):
        loop(lo, hi, back_a)

    def states():
        lax.fori_loop(0, NB, scan_up, jnp.zeros((128, 256), F32))

    def query_value_grads(lo, hi):
        loop(lo, hi, back_c)

    SCHEDULE = (
        (take_tokens,),
        (keys_of, 0, 1, 1),
        (w_step, 1, 0),
        (mixing, 0, 3),
        (w_step, 1, 1),
        (keys_of, -1, 2, 2),
        (mixing, 3, 7),
        (w_step, 2, 0),
        (mixing, 7, 12),
        (w_step, 2, 1),
        (mixing, 12, 16),
        (trails,),
        (key_grads, 0, 8),
        (w_step, 3, 0),
        (key_grads, 8, 16),
        (w_step, 3, 1),
        (keys_of, -3, 1, 2),
        (keys_of, 2, 1, 2),
        (take_key_grads,),
        (weight_plane, 0),
        (weight_ring, 0, 2),
        (weight_plane, 1),
        (weight_ring, 2, 3),
        (w_step, 4, 0),
        (keys_of, 4, 1, 1),
        (token_grads_partner, 0, 3),
        (take, 0, 4),
        (take, 1, 4),
        (line_pass, 0),
        (token_grads_partner, 3, 5),
        (take, 2, 4),
        (line_pass, 1),
        (send_keys, 0),
        (send_keys, 1),
        (token_grads_partner, 5, 8),
        (take, 0, 3),
        (take, 1, 3),
        (take, 2, 3),
        (line_sums,),
        (send_keys, 2),
        (take, 0, 2),
        (take, 1, 2),
        (token_grads, 0, 4),
        (take, 2, 2),
        (token_grads, 4, 8),
        (take, 0, 1),
        (take, 1, 1),
        (take, 2, 1),
        (column_sums,),
        (send_keys, 3),
        (plane_sums,),
        (finish_ring_part,),
        (finish_plane_part,),
        (take_keys,),
        (scores, 0, 8),
        (states,),
        (query_value_grads, 0, 8),
        (weight_out,),
    )
    for step in SCHEDULE:
        step[0](*step[1:])

    arrived(B.cot.at[0:30], B.cot_s.at[0])
    arrived(B.wall.at[0:7], B.w_s.at[0])
    tok_copy.wait_send()
    gt_copy.wait_send()
    arrived(B.gko.at[0:30], B.gk_s.at[0])
    arrived(B.keyi.at[0:30], B.key_s.at[0])

    @pl.when(jnp.logical_not(own_head_here))
    def _():
        arrived(B.gko.at[0:2], B.gk_s.at[1])
        arrived(B.keyi.at[0:2], B.key_s.at[1])

    arrived(B.dwz.at[0:7], B.rz_s.at[0])
    arrived(B.dwx.at[:, 0:3], B.r1_s.at[0])
    arrived(B.s1.at[:, 0:3], B.r2_s.at[0])
    arrived(B.px.at[0:15], B.px_s.at[0])
    arrived(B.zx.at[0:7], B.zx_s.at[0])
    arrived(B.fin.at[0:15], B.fin_s.at[0])


def write_out(*refs):
    ins, outs, sems = refs[:4], refs[4:8], refs[8]
    copies = [pltpu.make_async_copy(a, b, sems.at[i]) for i, (a, b) in enumerate(zip(ins, outs, strict=True))]
    for cp in copies:
        cp.start()
    for cp in copies:
        cp.wait()


def body(tokens, key_weight, queries, values, cotangent, log_decay):
    inside, across = tables()
    hbm, vmem = pl.BlockSpec(memory_space=pltpu.HBM), pl.BlockSpec(memory_space=pltpu.VMEM)
    shapes = [
        jax.ShapeDtypeStruct((256, WIDTH), BF16),
        jax.ShapeDtypeStruct((NB, 128, 128), BF16),
        jax.ShapeDtypeStruct((NB, 128, 256), BF16),
        jax.ShapeDtypeStruct((16, 8, WIDTH), F32),
    ]
    results = pl.pallas_call(
        kernel,
        out_shape=shapes,
        in_specs=[hbm] * 8,
        out_specs=[vmem] * 4,
        scratch_shapes=[pltpu.VMEM(shape, kind) for shape, kind in SCRATCH.values()]
        + [pltpu.SemaphoreType.DMA((n,)) for n in SEMS.values()]
        + [pltpu.SMEM((16,), F32)],
        compiler_params=pltpu.CompilerParams(
            collective_id=0, has_side_effects=True, vmem_limit_bytes=48 * 2**20
        ),
        name="retention",
    )(
        *(
            pltpu.with_memory_space_constraint(a, pltpu.HBM)
            for a in (
                log_decay,
                jnp.asarray(inside),
                jnp.asarray(across),
                tokens.reshape(256, WIDTH),
                key_weight,
                queries.reshape(NB, 128, 128),
                values.reshape(NB, 128, 256),
                cotangent.reshape(2, 128, 4096),
            )
        ),
    )
    gt, gq, gv, dw = pl.pallas_call(
        write_out,
        out_shape=shapes,
        in_specs=[vmem] * 4,
        out_specs=[hbm] * 4,
        scratch_shapes=[pltpu.SemaphoreType.DMA((4,))],
        compiler_params=pltpu.CompilerParams(vmem_limit_bytes=8 * 2**20),
        name="write_out",
    )(*results)
    return (
        gt.reshape(1, 256, WIDTH),
        gq.reshape(1, 4096, 1, 128),
        gv.reshape(1, 4096, 1, 256),
        dw.reshape(128, WIDTH),
    )


def solution(mesh):
    return jax.shard_map(
        body,
        mesh=mesh,
        in_specs=(
            P("dp", "sp", None),
            P("dp", None),
            P("dp", None, "sp", None),
            P("dp", None, "sp", None),
            P("dp", "sp", None),
            P(),
        ),
        out_specs=(
            P("dp", "sp", None),
            P("dp", None, "sp", None),
            P("dp", None, "sp", None),
            P("dp", None),
        ),
        check_vma=False,
    )
```

```python
import functools

import jax
import jax.numpy as jnp
import numpy as np
from jax import lax
from jax.experimental import pallas as pl
from jax.experimental.pallas import tpu as pltpu
from jax.sharding import PartitionSpec as P

MESH = pl.DeviceIdType.MESH
F32, BF16 = jnp.float32, jnp.bfloat16
BLOCK = 128
NB = 32
WIDTH = 2048
CHAINS, CW = 3, 256
C1 = CHAINS * CW
C2 = WIDTH - C1
H2 = C2 // 2
ORDERS = {
    "cot": ((1, 1), (3, 3), (3, 1), (1, 3), (2, 1), (2, 3), (1, 2), (3, 2), (2, 2), (1, 0), (3, 0), (0, 2), (2, 0), (0, 1), (0, 3), (0, 0)),
    "gk": ((1, 1), (3, 3), (3, 1), (1, 3), (2, 1), (2, 3), (1, 2), (3, 2), (2, 2), (1, 0), (3, 0), (0, 2), (2, 0), (0, 1), (0, 3), (0, 0)),
    "end": ((1, 1), (3, 3), (3, 1), (1, 3), (2, 1), (2, 3), (1, 2), (3, 2), (2, 2), (1, 0), (3, 0), (0, 2), (2, 0), (0, 1), (0, 3), (0, 0)),
}
FACTOR = BLOCK**-0.5


def tables():
    half = 64
    freq = 10000.0 ** (-np.arange(half, dtype=np.float64) / half)
    freq = np.concatenate([freq, freq])
    sign = np.where(np.arange(128) < half, -1.0, 1.0)
    ang_j = np.arange(128, dtype=np.float64)[:, None] * freq
    ang_n = 128.0 * np.arange(NB, dtype=np.float64)[:, None] * freq
    inside = np.stack([np.cos(ang_j), np.sin(ang_j), sign * np.cos(ang_j), sign * np.sin(ang_j)])
    across = np.stack([np.cos(ang_n), np.sin(ang_n)], axis=1)
    return inside.astype(np.float32), across.astype(np.float32)


def dot(a, b, ca, cb):
    return lax.dot_general(a, b, (((ca,), (cb,)), ((), ())), preferred_element_type=F32)


TARGETS = (
    ((2, 2), (0, 2), (1, 2), (3, 0), (1, 0), (3, 2), (2, 0), (0, 0)),
    ((2, 1), (0, 3), (1, 3), (3, 1), (1, 1), (3, 3), (2, 3), (0, 1)),
)

SCRATCH = dict(
    tok=((512, WIDTH), BF16),
    wall=((8, 128, WIDTH), BF16),
    vv=((NB, 128, 256), BF16),
    rq=((NB, 128, 128), BF16),
    dq=((NB, 128, 128), BF16),
    cosv=((NB, 128, 128), F32),
    sinv=((NB, 128, 128), F32),
    jtv=((4, 128, 128), F32),
    ntv=((NB, 2, 128), F32),
    within=((128, 128), F32),
    rise=((128, 128), F32),
    fall=((128, 128), F32),
    cot=((NB, 128, 256), BF16),
    mix=((NB, 128, 128), BF16),
    trl=((NB, 128, 256), F32),
    trb=((NB, 128, 256), BF16),
    entb=((NB, 128, 256), BF16),
    gko=((NB, 128, 128), BF16),
    gki=((4, 128, 1024), BF16),
    gkt=((1024, 512), BF16),
    keyo=((8, 4, 128, 128), BF16),
    keyi=((NB, 128, 128), BF16),
    gts=((256, WIDTH), BF16),
    gtr=((256, WIDTH), BF16),
    dwz=((8, 128, C1), BF16),
    rz=((CHAINS, 2, 4, 128, CW), BF16),
    dwx=((2, 4, 4, 8, 8, H2), BF16),
    f1=((2, 2, 2, 8, 8, H2), BF16),
    r1=((2, 2, 4, 8, 8, H2), BF16),
    s1=((2, 4, 8, 8, H2), BF16),
    r2=((2, 4, 8, 8, H2), BF16),
    zx=((2, 8, 8, H2), BF16),
    zr=((2, 8, 8, H2), BF16),
    px=((16, 8, C1), BF16),
    pr=((16, 8, C1), BF16),
    fin=((16, 8, WIDTH), BF16),
)
SEMS = dict(
    loc=7, cot_s=1, cot_r=16, tok_s=1, tok_r=1, w_s=1, wp_r=7, wm_r=7, gk_s=2, gk_r=1, key_s=2, key_r=16,
    gt_s=1, gt_r=1, rz_s=1, rz_r=8 * CHAINS, f1_r=4, r1_s=1, r1_r=2, r2_s=1, r2_r=2, zx_s=1, zx_r=2, px_s=1, px_r=1, fin_s=1, finx_r=2, finz_r=1,
)


def kernel(ld_ref, jt_ref, nt_ref, tok_ref, w_ref, q_ref, v_ref, cot_ref, gt_o, gq_o, gv_o, dw_o, *scratch):
    B = type("B", (), dict(zip([*SCRATCH, *SEMS, "lds"], scratch, strict=True)))
    sp, dp = lax.axis_index("sp"), lax.axis_index("dp")
    y, x = lax.div(sp, 4), lax.rem(sp, 4)
    z, c = lax.div(dp, 2), lax.rem(dp, 2)
    head_core = lax.rem(x, 2)
    head_at = lax.div(sp, 2)

    def plane(t, name="end"):
        if isinstance(t, int):
            dy, dx = ORDERS[name][t]
        else:
            code = jnp.int32(0)
            for k, (a, b) in enumerate(ORDERS[name][:15]):
                code = jnp.where(t == k, a * 4 + b, code)
            dy, dx = lax.div(code, 4), lax.rem(code, 4)
        to = lax.rem(y + dy, 4) * 4 + lax.rem(x + dx, 4)
        of = lax.rem(y + 4 - dy, 4) * 4 + lax.rem(x + 4 - dx, 4)
        return to, of

    def zat(dz):
        return lax.rem(z + 8 + dz, 8)

    def zdev(dz, core=c):
        return zat(dz) * 2 + core

    def remote(src, dst, ss, rs, dev):
        return pltpu.make_async_remote_copy(
            src_ref=src, dst_ref=dst, send_sem=ss, recv_sem=rs, device_id=dev, device_id_type=MESH
        )

    def arrived(ref, sem):
        pltpu.make_async_copy(ref, ref, sem).wait()

    def loop(lo, hi, f):
        def step(i, carry):
            f(i)
            return carry

        lax.fori_loop(lo, hi, step, 0)

    def lanes(i, width=128):
        return pl.ds(pl.multiple_of(i * width, width), width)

    bar = pltpu.get_barrier_semaphore()
    partner = (sp, zdev(0, 1 - c))

    def greet(k):
        for core in (c, 1 - c):
            pl.semaphore_signal(bar, inc=1, device_id=(lax.rem(sp + k, 16), zdev(0, core)), device_id_type=MESH)

    loop(1, 16, greet)
    pl.semaphore_signal(bar, inc=1, device_id=partner, device_id_type=MESH)
    loop(1, 8, lambda k: pl.semaphore_signal(bar, inc=1, device_id=(sp, zdev(k)), device_id_type=MESH))

    loads = [
        pltpu.make_async_copy(ld_ref, B.lds, B.loc.at[6]),
        pltpu.make_async_copy(q_ref, B.rq, B.loc.at[0]),
        pltpu.make_async_copy(v_ref, B.vv, B.loc.at[1]),
        pltpu.make_async_copy(tok_ref, B.tok.at[pl.ds(c * 256, 256)], B.loc.at[2]),
        pltpu.make_async_copy(w_ref, B.wall.at[z], B.loc.at[3]),
        pltpu.make_async_copy(jt_ref, B.jtv, B.loc.at[4]),
        pltpu.make_async_copy(nt_ref, B.ntv, B.loc.at[5]),
        pltpu.make_async_copy(cot_ref.at[:, :, lanes(sp, 256)], B.cot.at[pl.ds(2 * sp, 2)], B.cot_r.at[sp]),
    ]
    for cp in loads:
        cp.start()
    pl.semaphore_wait(bar, 38)

    up, down = (sp, zdev(1)), (sp, zdev(-1))

    def w_copy(k, part, way):
        at = zat(-k if way == 0 else k)
        rows = pl.ds(64 * part, 64)
        sem = (B.wp_r if way == 0 else B.wm_r).at[2 * k + part if k < 3 else 6]
        src = w_ref.at[rows] if k == 0 else B.wall.at[at, rows]
        return remote(src, B.wall.at[at, rows], B.w_s.at[0], sem, up if way == 0 else down)

    def w_step(k, part):
        for way in (0, 1):
            if k == 4:
                arrived(B.wall.at[zat(4), pl.ds(64 * way, 64)], (B.wp_r, B.wm_r)[way].at[6])
                continue
            at = zat(-k if way == 0 else k)
            arrived(B.wall.at[at, pl.ds(64 * part, 64)], (B.wp_r, B.wm_r)[way].at[2 * (k - 1) + part])
            if k < 3 or part == way:
                w_copy(k, part, way).start()

    for part in range(2):
        for way in (0, 1):
            w_copy(0, part, way).start()

    def cot_copy(t):
        to, _ = plane(t, "cot")
        return remote(
            cot_ref.at[:, :, lanes(to, 256)], B.cot.at[pl.ds(2 * sp, 2)], B.cot_s.at[0], B.cot_r.at[sp], (to, dp)
        )

    for t in range(15):
        cot_copy(t).start()
    tok_copy = remote(tok_ref, B.tok.at[pl.ds(c * 256, 256)], B.tok_s.at[0], B.tok_r.at[0], partner)
    tok_copy.start()

    loads[0].wait()
    ld = B.lds[sp]
    rows = lax.broadcasted_iota(jnp.int32, (128, 128), 0).astype(F32)
    cols = lax.broadcasted_iota(jnp.int32, (128, 128), 1).astype(F32)
    offset = rows - cols
    B.within[...] = jnp.where(offset >= 0, jnp.exp(jnp.maximum(offset, 0.0) * ld), 0.0)
    B.rise[...] = jnp.exp((rows + 1.0) * ld)
    B.fall[...] = jnp.exp((127.0 - rows) * ld)
    growth = jnp.exp(jnp.full((1, 256), 128.0, F32) * ld)
    loads[5].wait()
    loads[6].wait()
    loads[1].wait()

    def turn(n):
        cn, sn = B.ntv[n, 0:1, :], B.ntv[n, 1:2, :]
        cosine = cn * B.jtv[0] - sn * B.jtv[1]
        sine = sn * B.jtv[2] + cn * B.jtv[3]
        B.cosv[n] = cosine
        B.sinv[n] = sine
        u = B.rq[n].astype(F32)
        r = (u * cosine + pltpu.roll(u, 64, 1) * sine).astype(BF16)
        B.rq[n] = r
        B.dq[n] = (r.astype(F32) * B.rise[...]).astype(BF16)

    loop(0, NB, turn)

    def keys(hh):
        def part(i):
            k = dot(B.tok[pl.ds(pl.multiple_of(i * 256, 256), 256), :], B.wall[hh], 1, 1)
            B.keyo[hh, pl.ds(2 * i, 2)] = k.astype(BF16).reshape(2, 128, 128)

        loop(0, 2, part)

    def key_copy(hh, i, sem):
        return remote(
            B.keyo.at[hh, pl.ds(2 * i, 2)],
            B.keyi.at[pl.ds(2 * sp, 2)],
            B.key_s.at[sem],
            B.key_r.at[sp],
            (2 * hh + c, zdev(0, i)),
        )

    own_head_here = head_core == c

    def key_send(hh):
        for i in range(2):
            special = jnp.logical_and(hh == head_at, c == i)

            @pl.when(jnp.logical_and(special, own_head_here))
            def _():
                pltpu.make_async_copy(
                    B.keyo.at[hh, pl.ds(2 * i, 2)], B.keyi.at[pl.ds(2 * sp, 2)], B.key_r.at[sp]
                ).start()

            @pl.when(jnp.logical_and(special, jnp.logical_not(own_head_here)))
            def _():
                key_copy(hh, i, 1).start()

            @pl.when(jnp.logical_not(special))
            def _():
                key_copy(hh, i, 0).start()

    def cot_chunk(t):
        _, p = plane(t, "cot")
        arrived(B.cot.at[pl.ds(2 * p, 2)], B.cot_r.at[p])
        for b in range(2):
            n = 2 * p + b
            cb = B.cot[n]
            m = dot(cb, B.vv[n], 1, 1) * B.within[...]
            B.mix[n] = m.astype(BF16)
            B.trl[n] = dot(B.dq[n], cb, 0, 0)

    def take_tokens():
        loads[3].wait()
        arrived(B.tok.at[pl.ds((1 - c) * 256, 256)], B.tok_r.at[0])
        loads[4].wait()
        loads[2].wait()

    def keys_of(first, step, count):
        loop(0, count, lambda i: keys(zat(first + step * i)))

    def mixing(lo, hi):
        loop(lo, hi, cot_chunk)

    def scan(i, carry):
        n = NB - 1 - i
        B.trb[n] = carry.astype(BF16)
        return B.trl[n] + growth * carry

    def trails():
        lax.fori_loop(0, NB, scan, jnp.zeros((128, 256), F32))

    def gk_copy(t, sem=0):
        to, _ = plane(t, "gk")
        return remote(
            B.gko.at[pl.ds(2 * to, 2)],
            B.gki.at[pl.ds(2 * c, 2), :, lanes(head_at)],
            B.gk_s.at[sem],
            B.gk_r.at[0],
            (to, zdev(0, head_core)),
        )

    def gk_chunk(t):
        p, _ = plane(t, "gk")
        for b in range(2):
            n = 2 * p + b
            g = dot(B.mix[n], B.rq[n], 0, 0) + B.fall[...] * dot(B.vv[n], B.trb[n], 1, 1)
            g = g * B.cosv[n] - pltpu.roll(g, 64, 1) * B.sinv[n]
            B.gko[n] = (g * FACTOR).astype(BF16)

        @pl.when(t < 15)
        def _():
            gk_copy(t).start()

    def key_grads(lo, hi):
        loop(lo, hi, gk_chunk)
        if hi < 16:
            return

        @pl.when(own_head_here)
        def _():
            pltpu.make_async_copy(
                B.gko.at[pl.ds(2 * sp, 2)], B.gki.at[pl.ds(2 * c, 2), :, lanes(head_at)], B.gk_r.at[0]
            ).start()

        @pl.when(jnp.logical_not(own_head_here))
        def _():
            gk_copy(15, 1).start()

    def take_key_grads():
        arrived(B.gki, B.gk_r.at[0])
        for i in range(4):
            B.gkt[:, 128 * i : 128 * i + 128] = B.gki[i].T

    def send_keys(lo, hi):
        even = lax.rem(x + c, 2) == 0
        for (y0, x0), (y1, x1) in zip(TARGETS[0][lo:hi], TARGETS[1][lo:hi], strict=True):
            to = lax.rem(y + jnp.where(even, y0, y1), 4) * 4 + lax.rem(x + jnp.where(even, x0, x1), 4)
            key_send(lax.div(to, 2))

    def ring_refs(chain, way, k):
        at = pl.ds(chain * CW, CW)
        return at, B.rz.at[chain, way, k - 1], B.rz_r.at[(chain * 2 + way) * 4 + k - 1]

    def ring_send(chain, way, k):
        at, dst, sem = ring_refs(chain, way, k)
        d = zat(k if way == 0 else -k)
        remote(B.dwz.at[d, :, at], dst, B.rz_s.at[0], sem, up if way == 0 else down).start()

    def ring_take(chain, way, k):
        at, got, sem = ring_refs(chain, way, k)
        arrived(got, sem)
        if k == 1:
            return
        d = zat(k - 1 if way == 0 else 1 - k)

        def add(i):
            r = pl.ds(pl.multiple_of(i * 32, 32), 32)
            B.dwz[d, r, at] = (B.dwz[d, r, at].astype(F32) + got[r, :].astype(F32)).astype(BF16)

        loop(0, 4, add)
        ring_send(chain, way, k - 1)

    def take(chain, k):
        ring_take(chain, chain % 2, k)
        if k > 1:
            ring_take(chain, 1 - chain % 2, k - 1)

    def weight_ring(lo, hi):
        def tile(i):
            g = dot(B.gkt[...], B.tok[:, lanes(i, CW)], 1, 0)
            B.dwz[:, :, lanes(i, CW)] = g.astype(BF16).reshape(8, 128, CW)

        loop(lo, hi, tile)
        for chain in range(lo, hi):
            ring_send(chain, chain % 2, 4)
            ring_send(chain, 1 - chain % 2, 3)

    def line(way, step):
        if way == 0:
            at = lax.rem(x + step, 4)
            return at, x, (y * 4 + at, dp)
        at = lax.rem(y + step, 4)
        return at, y, (at * 4 + x, dp)

    def weight_plane(way):
        def tile(at, width):
            g = dot(B.gkt[...], B.tok[:, pl.ds(C1 + way * H2 + at, width)], 1, 0)
            g = g.astype(BF16).reshape(8, 4, 4, 8, width)
            for yy in range(4):
                for xx in range(4):
                    a1, a2 = (xx, yy) if way == 0 else (yy, xx)
                    B.dwx[way, a1, a2, :, :, pl.ds(at, width)] = g[:, yy, xx]

        if H2 % 256 == 0:
            loop(0, H2 // 256, lambda i: tile(pl.multiple_of(i * 256, 256), 256))
        else:
            for at in range(0, H2, 256):
                tile(at, min(256, H2 - at))
        for step in (1, 3):
            near, _, dev = line(way, step)
            far, _, _ = line(way, 2)
            side = 0 if step == 1 else 1
            through, own = pl.ds(2 * side, 2), pl.ds(2 - 2 * side, 2)
            remote(B.dwx.at[way, far, through], B.f1.at[way, side], B.r1_s.at[0], B.f1_r.at[2 * way + side], dev).start()
            remote(B.dwx.at[way, near, own], B.r1.at[way, side, own], B.r1_s.at[0], B.r1_r.at[way], dev).start()

    def line_pass(way):
        for step in (1, 3):
            near, _, dev = line(way, step)
            side = 0 if step == 1 else 1
            arrived(B.f1.at[way, side], B.f1_r.at[2 * way + side])

            def add(i):
                j, hh = lax.div(i, 4), lax.rem(i, 4) * 2
                have = B.dwx[way, near, 2 * side + j, pl.ds(hh, 2)].astype(F32)
                B.dwx[way, near, 2 * side + j, pl.ds(hh, 2)] = (have + B.f1[way, side, j, pl.ds(hh, 2)].astype(F32)).astype(BF16)

            loop(0, 8, add)
            through = pl.ds(2 * side, 2)
            remote(
                B.dwx.at[way, near, through], B.r1.at[way, side, through], B.r1_s.at[0], B.r1_r.at[way], dev
            ).start()

    def line_sums(way):
        arrived(B.r1.at[way], B.r1_r.at[way])
        me = (x, y)[way]

        def add(i):
            j, hh = lax.div(i, 4), lax.rem(i, 4) * 2
            total = B.dwx[way, me, j, pl.ds(hh, 2)].astype(F32)
            for side in range(2):
                total += B.r1[way, side, j, pl.ds(hh, 2)].astype(F32)
            B.s1[way, j, pl.ds(hh, 2)] = total.astype(BF16)

        loop(0, 16, add)
        for step in (2, 1, 3):
            at, here, dev = line(1 - way, step)
            remote(B.s1.at[way, at], B.r2.at[way, here], B.r2_s.at[0], B.r2_r.at[way], dev).start()

    def plane_sums(way):
        arrived(B.r2.at[way, 0:3], B.r2_r.at[way])
        B.r2[way, (y, x)[way]] = B.s1[way, (y, x)[way]]
        for hh in range(8):
            total = B.r2[way, 0, hh].astype(F32)
            for p in range(1, 4):
                total += B.r2[way, p, hh].astype(F32)
            B.zx[way, hh] = total.astype(BF16)
        for k in (4, 3, 5, 2, 6, 1, 7):
            d = zat(k)
            remote(B.zx.at[way, d], B.zr.at[way, z], B.zx_s.at[0], B.zx_r.at[way], (sp, zdev(k))).start()

    def own_rows(i):
        r = pl.ds(pl.multiple_of(i * 16, 16), 16)
        for chain in range(CHAINS):
            at = slice(chain * CW, chain * CW + CW)
            v = B.dwz[z, r, at].astype(F32) + B.rz[chain, 0, 0, r, :].astype(F32) + B.rz[chain, 1, 0, r, :].astype(F32)
            B.px[pl.ds(2 * i, 2), :, at] = v.reshape(2, 8, CW).astype(BF16)

    def column_sums():
        loop(0, 8, own_rows)
        for t in range(15):
            to, _ = plane(t)
            remote(B.px.at[to], B.pr.at[sp], B.px_s.at[0], B.px_r.at[0], (to, dp)).start()

    def total_of(ref, count):
        total = ref[0].astype(F32)
        for p in range(1, count):
            total += ref[p].astype(F32)
        return total.astype(BF16)

    def fin_send(lo, hi, sem):
        for t in range(15):
            to, _ = plane(t)
            ref = B.fin.at[sp, :, pl.ds(lo, hi - lo)]
            remote(ref, ref, B.fin_s.at[0], sem, (to, dp)).start()

    def finish_plane_part(way):
        arrived(B.zr.at[way, 0:7], B.zx_r.at[way])
        B.zr[way, z] = B.zx[way, z]
        lo = C1 + way * H2
        B.fin[sp, :, lo : lo + H2] = total_of(B.zr.at[way], 8)
        fin_send(lo, lo + H2, B.finx_r.at[way])

    def finish_ring_part():
        B.pr[sp] = B.px[sp]
        arrived(B.pr.at[0:15], B.px_r.at[0])
        B.fin[sp, :, 0:C1] = total_of(B.pr, 16)
        fin_send(0, C1, B.finz_r.at[0])

    def widen(j):
        dw_o[j] = B.fin[j].astype(F32)

    def weight_out():
        for way in (0, 1):
            arrived(B.fin.at[0:15, :, C1 + way * H2 : C1 + way * H2 + H2], B.finx_r.at[way])
        arrived(B.fin.at[0:15, :, 0:C1], B.finz_r.at[0])
        loop(0, 16, widen)

    def gt_tile(first):
        def tile(i):
            j = (1 - c) if first else c
            a = jnp.concatenate([B.gki[2 * j], B.gki[2 * j + 1]], axis=0)
            g = dot(a, B.wall[:, :, lanes(i, 256)].reshape(1024, 256), 1, 0)
            if first:
                B.gts[:, lanes(i, 256)] = g.astype(BF16)
            else:
                gt_o[:, lanes(i, 256)] = (g + B.gtr[:, lanes(i, 256)].astype(F32)).astype(BF16)

        return tile

    gt_copy = remote(B.gts, B.gtr, B.gt_s.at[0], B.gt_r.at[0], partner)

    def token_grads_partner(lo, hi):
        loop(lo, hi, gt_tile(True))
        if hi == 8:
            gt_copy.start()

    def token_grads(lo, hi):
        if lo == 0:
            arrived(B.gtr, B.gt_r.at[0])
        loop(lo, hi, gt_tile(False))

    def back_a(u):
        for cls in range(2):
            code = jnp.int32(0)
            for k, (dy, dx) in enumerate(TARGETS[cls]):
                code = jnp.where(u == k, (4 - dy) % 4 * 4 + (4 - dx) % 4, code)
            p = lax.rem(y + lax.div(code, 4), 4) * 4 + lax.rem(x + lax.rem(code, 4), 4)
            arrived(B.keyi.at[pl.ds(2 * p, 2)], B.key_r.at[p])
            for b in range(2):
                n = 2 * p + b
                k0 = B.keyi[n].astype(F32)
                rk = ((k0 * B.cosv[n] + pltpu.roll(k0, 64, 1) * B.sinv[n]) * FACTOR).astype(BF16)
                B.keyi[n] = rk
                B.dq[n] = (dot(B.rq[n], rk, 1, 1) * B.within[...]).astype(BF16)
                dk = (rk.astype(F32) * B.fall[...]).astype(BF16)
                B.trl[n] = dot(dk, B.vv[n], 0, 0)

    def scan_up(n, carry):
        B.entb[n] = carry.astype(BF16)
        return B.trl[n] + growth * carry

    def back_c(i):
        for b in range(4):
            n = 4 * i + b
            rk, cb, f = B.keyi[n], B.cot[n], B.fall[...]
            g = dot(B.mix[n], rk, 1, 0) + B.rise[...] * dot(cb, B.entb[n], 1, 1)
            gq_o[n] = (g * B.cosv[n] - pltpu.roll(g, 64, 1) * B.sinv[n]).astype(BF16)
            near, far = dot(B.dq[n], cb, 0, 0), dot(rk, B.trb[n], 1, 0)
            for h in range(2):
                at = slice(128 * h, 128 * h + 128)
                gv_o[n, :, at] = (near[:, at] + f * far[:, at]).astype(BF16)

    def scores(lo, hi):
        loop(lo, hi, back_a)

    def states():
        lax.fori_loop(0, NB, scan_up, jnp.zeros((128, 256), F32))

    def query_value_grads(lo, hi):
        loop(lo, hi, back_c)

    SCHEDULE = (
        (take_tokens,),
        (keys_of, 0, 1, 1),
        (w_step, 1, 0),
        (mixing, 0, 3),
        (w_step, 1, 1),
        (keys_of, -1, 2, 2),
        (mixing, 3, 7),
        (w_step, 2, 0),
        (mixing, 7, 12),
        (w_step, 2, 1),
        (mixing, 12, 16),
        (trails,),
        (key_grads, 0, 8),
        (w_step, 3, 0),
        (key_grads, 8, 16),
        (w_step, 3, 1),
        (keys_of, -3, 1, 2),
        (keys_of, 2, 1, 2),
        (take_key_grads,),
        (weight_plane, 0),
        (weight_ring, 0, 2),
        (weight_plane, 1),
        (weight_ring, 2, 3),
        (w_step, 4, 0),
        (keys_of, 4, 1, 1),
        (token_grads_partner, 0, 5),
        (take, 0, 4),
        (line_pass, 0),
        (take, 1, 4),
        (line_pass, 1),
        (take, 2, 4),
        (send_keys, 0, 1),
        (send_keys, 1, 2),
        (token_grads_partner, 5, 8),
        (take, 0, 3),
        (take, 1, 3),
        (take, 2, 3),
        (line_sums, 0),
        (send_keys, 2, 3),
        (send_keys, 3, 4),
        (take, 0, 2),
        (take, 1, 2),
        (take, 2, 2),
        (line_sums, 1),
        (send_keys, 4, 5),
        (send_keys, 5, 6),
        (take, 0, 1),
        (token_grads, 0, 3),
        (take, 1, 1),
        (take, 2, 1),
        (column_sums,),
        (send_keys, 6, 7),
        (send_keys, 7, 8),
        (scores, 0, 2),
        (plane_sums, 0),
        (scores, 2, 3),
        (plane_sums, 1),
        (token_grads, 3, 8),
        (scores, 3, 5),
        (finish_plane_part, 0),
        (finish_plane_part, 1),
        (finish_ring_part,),
        (scores, 5, 8),
        (states,),
        (query_value_grads, 0, 8),
        (weight_out,),
    )
    for step in SCHEDULE:
        step[0](*step[1:])

    arrived(B.cot.at[0:30], B.cot_s.at[0])
    arrived(B.wall.at[0:7], B.w_s.at[0])
    tok_copy.wait_send()
    gt_copy.wait_send()
    arrived(B.gko.at[0:30], B.gk_s.at[0])
    arrived(B.keyi.at[0:30], B.key_s.at[0])

    @pl.when(jnp.logical_not(own_head_here))
    def _():
        arrived(B.gko.at[0:2], B.gk_s.at[1])
        arrived(B.keyi.at[0:2], B.key_s.at[1])

    arrived(B.dwz.at[0:7], B.rz_s.at[0])
    arrived(B.dwx.at[:, 0:3], B.r1_s.at[0])
    arrived(B.s1.at[:, 0:3], B.r2_s.at[0])
    arrived(B.px.at[0:15], B.px_s.at[0])
    arrived(B.zx.at[:, 0:7], B.zx_s.at[0])
    arrived(B.fin.at[0:15], B.fin_s.at[0])


def write_out(*refs):
    ins, outs, sems = refs[:4], refs[4:8], refs[8]
    copies = [pltpu.make_async_copy(a, b, sems.at[i]) for i, (a, b) in enumerate(zip(ins, outs, strict=True))]
    for cp in copies:
        cp.start()
    for cp in copies:
        cp.wait()


def body(tokens, key_weight, queries, values, cotangent, log_decay):
    inside, across = tables()
    hbm, vmem = pl.BlockSpec(memory_space=pltpu.HBM), pl.BlockSpec(memory_space=pltpu.VMEM)
    shapes = [
        jax.ShapeDtypeStruct((256, WIDTH), BF16),
        jax.ShapeDtypeStruct((NB, 128, 128), BF16),
        jax.ShapeDtypeStruct((NB, 128, 256), BF16),
        jax.ShapeDtypeStruct((16, 8, WIDTH), F32),
    ]
    results = pl.pallas_call(
        kernel,
        out_shape=shapes,
        in_specs=[hbm] * 8,
        out_specs=[vmem] * 4,
        scratch_shapes=[pltpu.VMEM(shape, kind) for shape, kind in SCRATCH.values()]
        + [pltpu.SemaphoreType.DMA((n,)) for n in SEMS.values()]
        + [pltpu.SMEM((16,), F32)],
        compiler_params=pltpu.CompilerParams(
            collective_id=0, has_side_effects=True, vmem_limit_bytes=48 * 2**20
        ),
        name="retention",
    )(
        *(
            pltpu.with_memory_space_constraint(a, pltpu.HBM)
            for a in (
                log_decay,
                jnp.asarray(inside),
                jnp.asarray(across),
                tokens.reshape(256, WIDTH),
                key_weight,
                queries.reshape(NB, 128, 128),
                values.reshape(NB, 128, 256),
                cotangent.reshape(2, 128, 4096),
            )
        ),
    )
    gt, gq, gv, dw = pl.pallas_call(
        write_out,
        out_shape=shapes,
        in_specs=[vmem] * 4,
        out_specs=[hbm] * 4,
        scratch_shapes=[pltpu.SemaphoreType.DMA((4,))],
        compiler_params=pltpu.CompilerParams(vmem_limit_bytes=8 * 2**20),
        name="write_out",
    )(*results)
    return (
        gt.reshape(1, 256, WIDTH),
        gq.reshape(1, 4096, 1, 128),
        gv.reshape(1, 4096, 1, 256),
        dw.reshape(128, WIDTH),
    )


def solution(mesh):
    return jax.shard_map(
        body,
        mesh=mesh,
        in_specs=(
            P("dp", "sp", None),
            P("dp", None),
            P("dp", None, "sp", None),
            P("dp", None, "sp", None),
            P("dp", "sp", None),
            P(),
        ),
        out_specs=(
            P("dp", "sp", None),
            P("dp", None, "sp", None),
            P("dp", None, "sp", None),
            P("dp", None),
        ),
        check_vma=False,
    )
```

```python
import functools

import jax
import jax.numpy as jnp
import numpy as np
from jax import lax
from jax.experimental import pallas as pl
from jax.experimental.pallas import tpu as pltpu
from jax.sharding import PartitionSpec as P

MESH = pl.DeviceIdType.MESH
F32, BF16 = jnp.float32, jnp.bfloat16
BLOCK = 128
NB = 32
WIDTH = 2048
CHAINS, CW = 3, 256
C1 = CHAINS * CW
C2 = WIDTH - C1
H2 = C2 // 2
ORDERS = {
    "cot": ((1, 1), (3, 3), (3, 1), (1, 3), (2, 1), (2, 3), (1, 2), (3, 2), (2, 2), (1, 0), (3, 0), (0, 2), (2, 0), (0, 1), (0, 3), (0, 0)),
    "gk": ((1, 1), (3, 3), (3, 1), (1, 3), (2, 1), (2, 3), (1, 2), (3, 2), (2, 2), (1, 0), (3, 0), (0, 2), (2, 0), (0, 1), (0, 3), (0, 0)),
    "end": ((1, 1), (3, 3), (3, 1), (1, 3), (2, 1), (2, 3), (1, 2), (3, 2), (2, 2), (1, 0), (3, 0), (0, 2), (2, 0), (0, 1), (0, 3), (0, 0)),
}
FACTOR = BLOCK**-0.5


def tables():
    half = 64
    freq = 10000.0 ** (-np.arange(half, dtype=np.float64) / half)
    freq = np.concatenate([freq, freq])
    sign = np.where(np.arange(128) < half, -1.0, 1.0)
    ang_j = np.arange(128, dtype=np.float64)[:, None] * freq
    ang_n = 128.0 * np.arange(NB, dtype=np.float64)[:, None] * freq
    inside = np.stack([np.cos(ang_j), np.sin(ang_j), sign * np.cos(ang_j), sign * np.sin(ang_j)])
    across = np.stack([np.cos(ang_n), np.sin(ang_n)], axis=1)
    return inside.astype(np.float32), across.astype(np.float32)


def dot(a, b, ca, cb):
    return lax.dot_general(a, b, (((ca,), (cb,)), ((), ())), preferred_element_type=F32)


TARGETS = (
    ((2, 2), (0, 2), (1, 2), (3, 0), (1, 0), (3, 2), (2, 0), (0, 0)),
    ((2, 1), (0, 3), (1, 3), (3, 1), (1, 1), (3, 3), (2, 3), (0, 1)),
)

SCRATCH = dict(
    tok=((512, WIDTH), BF16),
    wall=((8, 128, WIDTH), BF16),
    vv=((NB, 128, 256), BF16),
    rq=((NB, 128, 128), BF16),
    dq=((NB, 128, 128), BF16),
    cosv=((NB, 128, 128), F32),
    sinv=((NB, 128, 128), F32),
    jtv=((4, 128, 128), F32),
    ntv=((NB, 2, 128), F32),
    within=((128, 128), F32),
    rise=((128, 128), F32),
    fall=((128, 128), F32),
    cot=((NB, 128, 256), BF16),
    mix=((NB, 128, 128), BF16),
    trl=((NB, 128, 256), F32),
    trb=((NB, 128, 256), BF16),
    entb=((NB, 128, 256), BF16),
    gko=((NB, 128, 128), BF16),
    gki=((4, 128, 1024), BF16),
    gkt=((1024, 512), BF16),
    keyo=((8, 4, 128, 128), BF16),
    keyi=((NB, 128, 128), BF16),
    gts=((256, WIDTH), BF16),
    gtr=((256, WIDTH), BF16),
    dwz=((8, 128, C1), BF16),
    rz=((CHAINS, 2, 4, 128, CW), BF16),
    dwx=((2, 4, 4, 8, 8, H2), BF16),
    f1=((2, 2, 2, 8, 8, H2), BF16),
    r1=((2, 2, 4, 8, 8, H2), BF16),
    s1=((2, 4, 8, 8, H2), BF16),
    r2=((2, 4, 8, 8, H2), BF16),
    zx=((2, 8, 8, H2), BF16),
    zr=((2, 8, 8, H2), BF16),
    px=((16, 8, C1), BF16),
    pr=((16, 8, C1), BF16),
    fin=((16, 8, WIDTH), BF16),
)
SEMS = dict(
    loc=7, cot_s=1, cot_r=16, tok_s=1, tok_r=1, w_s=1, wp_r=7, wm_r=7, gk_s=2, gk_r=1, key_s=2, key_r=16,
    gt_s=1, gt_r=1, rz_s=1, rz_r=8 * CHAINS, f1_r=4, r1_s=1, r1_r=2, r2_s=1, r2_r=2, zx_s=1, zx_r=2, px_s=1, px_r=1, fin_s=1, finx_r=2, finz_r=1,
)


def kernel(ld_ref, jt_ref, nt_ref, tok_ref, w_ref, q_ref, v_ref, cot_ref, gt_o, gq_o, gv_o, dw_o, *scratch):
    B = type("B", (), dict(zip([*SCRATCH, *SEMS, "lds"], scratch, strict=True)))
    sp, dp = lax.axis_index("sp"), lax.axis_index("dp")
    y, x = lax.div(sp, 4), lax.rem(sp, 4)
    z, c = lax.div(dp, 2), lax.rem(dp, 2)
    head_core = lax.rem(x, 2)
    head_at = lax.div(sp, 2)

    def plane(t, name="end"):
        if isinstance(t, int):
            dy, dx = ORDERS[name][t]
        else:
            code = jnp.int32(0)
            for k, (a, b) in enumerate(ORDERS[name][:15]):
                code = jnp.where(t == k, a * 4 + b, code)
            dy, dx = lax.div(code, 4), lax.rem(code, 4)
        to = lax.rem(y + dy, 4) * 4 + lax.rem(x + dx, 4)
        of = lax.rem(y + 4 - dy, 4) * 4 + lax.rem(x + 4 - dx, 4)
        return to, of

    def zat(dz):
        return lax.rem(z + 8 + dz, 8)

    def zdev(dz, core=c):
        return zat(dz) * 2 + core

    def remote(src, dst, ss, rs, dev):
        return pltpu.make_async_remote_copy(
            src_ref=src, dst_ref=dst, send_sem=ss, recv_sem=rs, device_id=dev, device_id_type=MESH
        )

    def arrived(ref, sem):
        pltpu.make_async_copy(ref, ref, sem).wait()

    def loop(lo, hi, f):
        def step(i, carry):
            f(i)
            return carry

        lax.fori_loop(lo, hi, step, 0)

    def lanes(i, width=128):
        return pl.ds(pl.multiple_of(i * width, width), width)

    bar = pltpu.get_barrier_semaphore()
    partner = (sp, zdev(0, 1 - c))

    def greet(k):
        for core in (c, 1 - c):
            pl.semaphore_signal(bar, inc=1, device_id=(lax.rem(sp + k, 16), zdev(0, core)), device_id_type=MESH)

    loop(1, 16, greet)
    pl.semaphore_signal(bar, inc=1, device_id=partner, device_id_type=MESH)
    loop(1, 8, lambda k: pl.semaphore_signal(bar, inc=1, device_id=(sp, zdev(k)), device_id_type=MESH))

    loads = [
        pltpu.make_async_copy(ld_ref, B.lds, B.loc.at[6]),
        pltpu.make_async_copy(q_ref, B.rq, B.loc.at[0]),
        pltpu.make_async_copy(v_ref, B.vv, B.loc.at[1]),
        pltpu.make_async_copy(tok_ref, B.tok.at[pl.ds(c * 256, 256)], B.loc.at[2]),
        pltpu.make_async_copy(w_ref, B.wall.at[z], B.loc.at[3]),
        pltpu.make_async_copy(jt_ref, B.jtv, B.loc.at[4]),
        pltpu.make_async_copy(nt_ref, B.ntv, B.loc.at[5]),
        pltpu.make_async_copy(cot_ref.at[:, :, lanes(sp, 256)], B.cot.at[pl.ds(2 * sp, 2)], B.cot_r.at[sp]),
    ]
    for cp in loads:
        cp.start()
    pl.semaphore_wait(bar, 38)

    up, down = (sp, zdev(1)), (sp, zdev(-1))

    def w_copy(k, part, way):
        at = zat(-k if way == 0 else k)
        rows = pl.ds(64 * part, 64)
        sem = (B.wp_r if way == 0 else B.wm_r).at[2 * k + part if k < 3 else 6]
        src = w_ref.at[rows] if k == 0 else B.wall.at[at, rows]
        return remote(src, B.wall.at[at, rows], B.w_s.at[0], sem, up if way == 0 else down)

    def w_step(k, part):
        for way in (0, 1):
            if k == 4:
                arrived(B.wall.at[zat(4), pl.ds(64 * way, 64)], (B.wp_r, B.wm_r)[way].at[6])
                continue
            at = zat(-k if way == 0 else k)
            arrived(B.wall.at[at, pl.ds(64 * part, 64)], (B.wp_r, B.wm_r)[way].at[2 * (k - 1) + part])
            if k < 3 or part == way:
                w_copy(k, part, way).start()

    for part in range(2):
        for way in (0, 1):
            w_copy(0, part, way).start()

    def cot_copy(t):
        to, _ = plane(t, "cot")
        return remote(
            cot_ref.at[:, :, lanes(to, 256)], B.cot.at[pl.ds(2 * sp, 2)], B.cot_s.at[0], B.cot_r.at[sp], (to, dp)
        )

    for t in range(15):
        cot_copy(t).start()
    tok_copy = remote(tok_ref, B.tok.at[pl.ds(c * 256, 256)], B.tok_s.at[0], B.tok_r.at[0], partner)
    tok_copy.start()

    loads[0].wait()
    ld = B.lds[sp]
    rows = lax.broadcasted_iota(jnp.int32, (128, 128), 0).astype(F32)
    cols = lax.broadcasted_iota(jnp.int32, (128, 128), 1).astype(F32)
    offset = rows - cols
    B.within[...] = jnp.where(offset >= 0, jnp.exp(jnp.maximum(offset, 0.0) * ld), 0.0)
    B.rise[...] = jnp.exp((rows + 1.0) * ld)
    B.fall[...] = jnp.exp((127.0 - rows) * ld)
    growth = jnp.exp(jnp.full((1, 256), 128.0, F32) * ld)
    loads[5].wait()
    loads[6].wait()
    loads[1].wait()

    def turn(n):
        cn, sn = B.ntv[n, 0:1, :], B.ntv[n, 1:2, :]
        cosine = cn * B.jtv[0] - sn * B.jtv[1]
        sine = sn * B.jtv[2] + cn * B.jtv[3]
        B.cosv[n] = cosine
        B.sinv[n] = sine
        u = B.rq[n].astype(F32)
        r = (u * cosine + pltpu.roll(u, 64, 1) * sine).astype(BF16)
        B.rq[n] = r
        B.dq[n] = (r.astype(F32) * B.rise[...]).astype(BF16)

    loop(0, NB, turn)

    def keys(hh):
        def part(i):
            k = dot(B.tok[pl.ds(pl.multiple_of(i * 256, 256), 256), :], B.wall[hh], 1, 1)
            B.keyo[hh, pl.ds(2 * i, 2)] = k.astype(BF16).reshape(2, 128, 128)

        loop(0, 2, part)

    def key_copy(hh, i, sem):
        return remote(
            B.keyo.at[hh, pl.ds(2 * i, 2)],
            B.keyi.at[pl.ds(2 * sp, 2)],
            B.key_s.at[sem],
            B.key_r.at[sp],
            (2 * hh + c, zdev(0, i)),
        )

    own_head_here = head_core == c

    def key_send(hh):
        for i in range(2):
            special = jnp.logical_and(hh == head_at, c == i)

            @pl.when(jnp.logical_and(special, own_head_here))
            def _():
                pltpu.make_async_copy(
                    B.keyo.at[hh, pl.ds(2 * i, 2)], B.keyi.at[pl.ds(2 * sp, 2)], B.key_r.at[sp]
                ).start()

            @pl.when(jnp.logical_and(special, jnp.logical_not(own_head_here)))
            def _():
                key_copy(hh, i, 1).start()

            @pl.when(jnp.logical_not(special))
            def _():
                key_copy(hh, i, 0).start()

    def cot_chunk(t):
        _, p = plane(t, "cot")
        arrived(B.cot.at[pl.ds(2 * p, 2)], B.cot_r.at[p])
        for b in range(2):
            n = 2 * p + b
            cb = B.cot[n]
            m = dot(cb, B.vv[n], 1, 1) * B.within[...]
            B.mix[n] = m.astype(BF16)
            B.trl[n] = dot(B.dq[n], cb, 0, 0)

    def take_tokens():
        loads[3].wait()
        arrived(B.tok.at[pl.ds((1 - c) * 256, 256)], B.tok_r.at[0])
        loads[4].wait()
        loads[2].wait()

    def keys_of(first, step, count):
        loop(0, count, lambda i: keys(zat(first + step * i)))

    def mixing(lo, hi):
        loop(lo, hi, cot_chunk)

    def scan(i, carry):
        n = NB - 1 - i
        B.trb[n] = carry.astype(BF16)
        return B.trl[n] + growth * carry

    def trails():
        lax.fori_loop(0, NB, scan, jnp.zeros((128, 256), F32))

    def gk_copy(t, sem=0):
        to, _ = plane(t, "gk")
        return remote(
            B.gko.at[pl.ds(2 * to, 2)],
            B.gki.at[pl.ds(2 * c, 2), :, lanes(head_at)],
            B.gk_s.at[sem],
            B.gk_r.at[0],
            (to, zdev(0, head_core)),
        )

    def gk_chunk(t):
        p, _ = plane(t, "gk")
        for b in range(2):
            n = 2 * p + b
            g = dot(B.mix[n], B.rq[n], 0, 0) + B.fall[...] * dot(B.vv[n], B.trb[n], 1, 1)
            g = g * B.cosv[n] - pltpu.roll(g, 64, 1) * B.sinv[n]
            B.gko[n] = (g * FACTOR).astype(BF16)

        @pl.when(t < 15)
        def _():
            gk_copy(t).start()

    def key_grads(lo, hi):
        loop(lo, hi, gk_chunk)
        if hi < 16:
            return

        @pl.when(own_head_here)
        def _():
            pltpu.make_async_copy(
                B.gko.at[pl.ds(2 * sp, 2)], B.gki.at[pl.ds(2 * c, 2), :, lanes(head_at)], B.gk_r.at[0]
            ).start()

        @pl.when(jnp.logical_not(own_head_here))
        def _():
            gk_copy(15, 1).start()

    def take_key_grads():
        arrived(B.gki, B.gk_r.at[0])
        for i in range(4):
            B.gkt[:, 128 * i : 128 * i + 128] = B.gki[i].T

    def send_keys(lo, hi):
        even = lax.rem(x + c, 2) == 0
        for (y0, x0), (y1, x1) in zip(TARGETS[0][lo:hi], TARGETS[1][lo:hi], strict=True):
            to = lax.rem(y + jnp.where(even, y0, y1), 4) * 4 + lax.rem(x + jnp.where(even, x0, x1), 4)
            key_send(lax.div(to, 2))

    def ring_refs(chain, way, k):
        at = pl.ds(chain * CW, CW)
        return at, B.rz.at[chain, way, k - 1], B.rz_r.at[(chain * 2 + way) * 4 + k - 1]

    def ring_send(chain, way, k):
        at, dst, sem = ring_refs(chain, way, k)
        d = zat(k if way == 0 else -k)
        remote(B.dwz.at[d, :, at], dst, B.rz_s.at[0], sem, up if way == 0 else down).start()

    def ring_take(chain, way, k):
        at, got, sem = ring_refs(chain, way, k)
        arrived(got, sem)
        if k == 1:
            return
        d = zat(k - 1 if way == 0 else 1 - k)

        def add(i):
            r = pl.ds(pl.multiple_of(i * 32, 32), 32)
            B.dwz[d, r, at] = (B.dwz[d, r, at].astype(F32) + got[r, :].astype(F32)).astype(BF16)

        loop(0, 4, add)
        ring_send(chain, way, k - 1)

    def take(chain, k):
        ring_take(chain, chain % 2, k)
        if k > 1:
            ring_take(chain, 1 - chain % 2, k - 1)

    def weight_ring(lo, hi):
        def tile(i):
            g = dot(B.gkt[...], B.tok[:, lanes(i, CW)], 1, 0)
            B.dwz[:, :, lanes(i, CW)] = g.astype(BF16).reshape(8, 128, CW)

        loop(lo, hi, tile)
        for chain in range(lo, hi):
            ring_send(chain, chain % 2, 4)
            ring_send(chain, 1 - chain % 2, 3)

    def line(way, step):
        if way == 0:
            at = lax.rem(x + step, 4)
            return at, x, (y * 4 + at, dp)
        at = lax.rem(y + step, 4)
        return at, y, (at * 4 + x, dp)

    def weight_plane(way):
        def tile(at, width):
            g = dot(B.gkt[...], B.tok[:, pl.ds(C1 + way * H2 + at, width)], 1, 0)
            g = g.astype(BF16).reshape(8, 4, 4, 8, width)
            for yy in range(4):
                for xx in range(4):
                    a1, a2 = (xx, yy) if way == 0 else (yy, xx)
                    B.dwx[way, a1, a2, :, :, pl.ds(at, width)] = g[:, yy, xx]

        if H2 % 256 == 0:
            loop(0, H2 // 256, lambda i: tile(pl.multiple_of(i * 256, 256), 256))
        else:
            for at in range(0, H2, 256):
                tile(at, min(256, H2 - at))
        for step in (1, 3):
            near, _, dev = line(way, step)
            far, _, _ = line(way, 2)
            side = 0 if step == 1 else 1
            through, own = pl.ds(2 * side, 2), pl.ds(2 - 2 * side, 2)
            remote(B.dwx.at[way, far, through], B.f1.at[way, side], B.r1_s.at[0], B.f1_r.at[2 * way + side], dev).start()
            remote(B.dwx.at[way, near, own], B.r1.at[way, side, own], B.r1_s.at[0], B.r1_r.at[way], dev).start()

    def line_pass(way):
        for step in (1, 3):
            near, _, dev = line(way, step)
            side = 0 if step == 1 else 1
            arrived(B.f1.at[way, side], B.f1_r.at[2 * way + side])

            def add(i):
                j, hh = lax.div(i, 4), lax.rem(i, 4) * 2
                have = B.dwx[way, near, 2 * side + j, pl.ds(hh, 2)].astype(F32)
                B.dwx[way, near, 2 * side + j, pl.ds(hh, 2)] = (have + B.f1[way, side, j, pl.ds(hh, 2)].astype(F32)).astype(BF16)

            loop(0, 8, add)
            through = pl.ds(2 * side, 2)
            remote(
                B.dwx.at[way, near, through], B.r1.at[way, side, through], B.r1_s.at[0], B.r1_r.at[way], dev
            ).start()

    def line_sums(way):
        arrived(B.r1.at[way], B.r1_r.at[way])
        me = (x, y)[way]

        def add(i):
            j, hh = lax.div(i, 4), lax.rem(i, 4) * 2
            total = B.dwx[way, me, j, pl.ds(hh, 2)].astype(F32)
            for side in range(2):
                total += B.r1[way, side, j, pl.ds(hh, 2)].astype(F32)
            B.s1[way, j, pl.ds(hh, 2)] = total.astype(BF16)

        loop(0, 16, add)
        for step in (2, 1, 3):
            at, here, dev = line(1 - way, step)
            remote(B.s1.at[way, at], B.r2.at[way, here], B.r2_s.at[0], B.r2_r.at[way], dev).start()

    def plane_sums(way):
        arrived(B.r2.at[way, 0:3], B.r2_r.at[way])
        B.r2[way, (y, x)[way]] = B.s1[way, (y, x)[way]]
        for hh in range(8):
            total = B.r2[way, 0, hh].astype(F32)
            for p in range(1, 4):
                total += B.r2[way, p, hh].astype(F32)
            B.zx[way, hh] = total.astype(BF16)
        for k in (4, 3, 5, 2, 6, 1, 7):
            d = zat(k)
            remote(B.zx.at[way, d], B.zr.at[way, z], B.zx_s.at[0], B.zx_r.at[way], (sp, zdev(k))).start()

    def own_rows(i):
        r = pl.ds(pl.multiple_of(i * 16, 16), 16)
        for chain in range(CHAINS):
            at = slice(chain * CW, chain * CW + CW)
            v = B.dwz[z, r, at].astype(F32) + B.rz[chain, 0, 0, r, :].astype(F32) + B.rz[chain, 1, 0, r, :].astype(F32)
            B.px[pl.ds(2 * i, 2), :, at] = v.reshape(2, 8, CW).astype(BF16)

    def column_sums():
        loop(0, 8, own_rows)
        for t in range(15):
            to, _ = plane(t)
            remote(B.px.at[to], B.pr.at[sp], B.px_s.at[0], B.px_r.at[0], (to, dp)).start()

    def total_of(ref, count):
        total = ref[0].astype(F32)
        for p in range(1, count):
            total += ref[p].astype(F32)
        return total.astype(BF16)

    def fin_send(lo, hi, sem):
        for t in range(15):
            to, _ = plane(t)
            ref = B.fin.at[sp, :, pl.ds(lo, hi - lo)]
            remote(ref, ref, B.fin_s.at[0], sem, (to, dp)).start()

    def finish_plane_part(way):
        arrived(B.zr.at[way, 0:7], B.zx_r.at[way])
        B.zr[way, z] = B.zx[way, z]
        lo = C1 + way * H2
        B.fin[sp, :, lo : lo + H2] = total_of(B.zr.at[way], 8)
        fin_send(lo, lo + H2, B.finx_r.at[way])

    def finish_ring_part():
        B.pr[sp] = B.px[sp]
        arrived(B.pr.at[0:15], B.px_r.at[0])
        B.fin[sp, :, 0:C1] = total_of(B.pr, 16)
        fin_send(0, C1, B.finz_r.at[0])

    def widen(j):
        dw_o[j] = B.fin[j].astype(F32)

    def weight_out():
        for way in (0, 1):
            arrived(B.fin.at[0:15, :, C1 + way * H2 : C1 + way * H2 + H2], B.finx_r.at[way])
        arrived(B.fin.at[0:15, :, 0:C1], B.finz_r.at[0])
        loop(0, 16, widen)

    def gt_tile(first):
        def tile(i):
            j = (1 - c) if first else c
            a = jnp.concatenate([B.gki[2 * j], B.gki[2 * j + 1]], axis=0)
            g = dot(a, B.wall[:, :, lanes(i, 256)].reshape(1024, 256), 1, 0)
            if first:
                B.gts[:, lanes(i, 256)] = g.astype(BF16)
            else:
                gt_o[:, lanes(i, 256)] = (g + B.gtr[:, lanes(i, 256)].astype(F32)).astype(BF16)

        return tile

    gt_copy = remote(B.gts, B.gtr, B.gt_s.at[0], B.gt_r.at[0], partner)

    def token_grads_partner(lo, hi):
        loop(lo, hi, gt_tile(True))
        if hi == 8:
            gt_copy.start()

    def token_grads(lo, hi):
        if lo == 0:
            arrived(B.gtr, B.gt_r.at[0])
        loop(lo, hi, gt_tile(False))

    def back_a(u):
        for cls in range(2):
            code = jnp.int32(0)
            for k, (dy, dx) in enumerate(TARGETS[cls]):
                code = jnp.where(u == k, (4 - dy) % 4 * 4 + (4 - dx) % 4, code)
            p = lax.rem(y + lax.div(code, 4), 4) * 4 + lax.rem(x + lax.rem(code, 4), 4)
            arrived(B.keyi.at[pl.ds(2 * p, 2)], B.key_r.at[p])
            for b in range(2):
                n = 2 * p + b
                k0 = B.keyi[n].astype(F32)
                rk = ((k0 * B.cosv[n] + pltpu.roll(k0, 64, 1) * B.sinv[n]) * FACTOR).astype(BF16)
                B.keyi[n] = rk
                B.dq[n] = (dot(B.rq[n], rk, 1, 1) * B.within[...]).astype(BF16)
                dk = (rk.astype(F32) * B.fall[...]).astype(BF16)
                B.trl[n] = dot(dk, B.vv[n], 0, 0)

    def scan_up(n, carry):
        B.entb[n] = carry.astype(BF16)
        return B.trl[n] + growth * carry

    def back_c(i):
        for b in range(4):
            n = 4 * i + b
            rk, cb, f = B.keyi[n], B.cot[n], B.fall[...]
            g = dot(B.mix[n], rk, 1, 0) + B.rise[...] * dot(cb, B.entb[n], 1, 1)
            gq_o[n] = (g * B.cosv[n] - pltpu.roll(g, 64, 1) * B.sinv[n]).astype(BF16)
            near, far = dot(B.dq[n], cb, 0, 0), dot(rk, B.trb[n], 1, 0)
            for h in range(2):
                at = slice(128 * h, 128 * h + 128)
                gv_o[n, :, at] = (near[:, at] + f * far[:, at]).astype(BF16)

    def scores(lo, hi):
        loop(lo, hi, back_a)

    def states():
        lax.fori_loop(0, NB, scan_up, jnp.zeros((128, 256), F32))

    def query_value_grads(lo, hi):
        loop(lo, hi, back_c)

    SCHEDULE = (
        (take_tokens,),
        (keys_of, 0, 1, 1),
        (w_step, 1, 0),
        (mixing, 0, 3),
        (w_step, 1, 1),
        (keys_of, -1, 2, 2),
        (mixing, 3, 7),
        (w_step, 2, 0),
        (mixing, 7, 12),
        (w_step, 2, 1),
        (mixing, 12, 16),
        (trails,),
        (key_grads, 0, 8),
        (w_step, 3, 0),
        (key_grads, 8, 16),
        (w_step, 3, 1),
        (keys_of, -3, 1, 2),
        (keys_of, 2, 1, 2),
        (take_key_grads,),
        (weight_plane, 0),
        (weight_ring, 0, 2),
        (weight_plane, 1),
        (weight_ring, 2, 3),
        (w_step, 4, 0),
        (keys_of, 4, 1, 1),
        (token_grads_partner, 0, 5),
        (take, 0, 4),
        (line_pass, 0),
        (take, 1, 4),
        (line_pass, 1),
        (take, 2, 4),
        (send_keys, 0, 1),
        (send_keys, 1, 2),
        (token_grads_partner, 5, 8),
        (take, 0, 3),
        (take, 1, 3),
        (take, 2, 3),
        (line_sums, 0),
        (send_keys, 2, 3),
        (send_keys, 3, 4),
        (take, 0, 2),
        (take, 1, 2),
        (take, 2, 2),
        (line_sums, 1),
        (send_keys, 4, 5),
        (send_keys, 5, 6),
        (take, 0, 1),
        (token_grads, 0, 3),
        (take, 1, 1),
        (take, 2, 1),
        (column_sums,),
        (send_keys, 6, 7),
        (send_keys, 7, 8),
        (scores, 0, 2),
        (plane_sums, 0),
        (scores, 2, 3),
        (plane_sums, 1),
        (token_grads, 3, 6),
        (finish_ring_part,),
        (scores, 3, 4),
        (finish_plane_part, 0),
        (scores, 4, 5),
        (finish_plane_part, 1),
        (scores, 5, 8),
        (states,),
        (token_grads, 6, 8),
        (query_value_grads, 0, 8),
        (weight_out,),
    )
    for step in SCHEDULE:
        step[0](*step[1:])

    arrived(B.cot.at[0:30], B.cot_s.at[0])
    arrived(B.wall.at[0:7], B.w_s.at[0])
    tok_copy.wait_send()
    gt_copy.wait_send()
    arrived(B.gko.at[0:30], B.gk_s.at[0])
    arrived(B.keyi.at[0:30], B.key_s.at[0])

    @pl.when(jnp.logical_not(own_head_here))
    def _():
        arrived(B.gko.at[0:2], B.gk_s.at[1])
        arrived(B.keyi.at[0:2], B.key_s.at[1])

    arrived(B.dwz.at[0:7], B.rz_s.at[0])
    arrived(B.dwx.at[:, 0:3], B.r1_s.at[0])
    arrived(B.s1.at[:, 0:3], B.r2_s.at[0])
    arrived(B.px.at[0:15], B.px_s.at[0])
    arrived(B.zx.at[:, 0:7], B.zx_s.at[0])
    arrived(B.fin.at[0:15], B.fin_s.at[0])


def write_out(*refs):
    ins, outs, sems = refs[:4], refs[4:8], refs[8]
    copies = []
    for a, b in zip(ins, outs, strict=True):
        rows = a.shape[0] // 4
        for i in range(4):
            at = pl.ds(i * rows, rows)
            copies.append(pltpu.make_async_copy(a.at[at], b.at[at], sems.at[len(copies)]))
    for cp in copies:
        cp.start()
    for cp in copies:
        cp.wait()


def body(tokens, key_weight, queries, values, cotangent, log_decay):
    inside, across = tables()
    hbm, vmem = pl.BlockSpec(memory_space=pltpu.HBM), pl.BlockSpec(memory_space=pltpu.VMEM)
    shapes = [
        jax.ShapeDtypeStruct((256, WIDTH), BF16),
        jax.ShapeDtypeStruct((NB, 128, 128), BF16),
        jax.ShapeDtypeStruct((NB, 128, 256), BF16),
        jax.ShapeDtypeStruct((16, 8, WIDTH), F32),
    ]
    results = pl.pallas_call(
        kernel,
        out_shape=shapes,
        in_specs=[hbm] * 8,
        out_specs=[vmem] * 4,
        scratch_shapes=[pltpu.VMEM(shape, kind) for shape, kind in SCRATCH.values()]
        + [pltpu.SemaphoreType.DMA((n,)) for n in SEMS.values()]
        + [pltpu.SMEM((16,), F32)],
        compiler_params=pltpu.CompilerParams(
            collective_id=0, has_side_effects=True, vmem_limit_bytes=48 * 2**20
        ),
        name="retention",
    )(
        *(
            pltpu.with_memory_space_constraint(a, pltpu.HBM)
            for a in (
                log_decay,
                jnp.asarray(inside),
                jnp.asarray(across),
                tokens.reshape(256, WIDTH),
                key_weight,
                queries.reshape(NB, 128, 128),
                values.reshape(NB, 128, 256),
                cotangent.reshape(2, 128, 4096),
            )
        ),
    )
    gt, gq, gv, dw = pl.pallas_call(
        write_out,
        out_shape=shapes,
        in_specs=[vmem] * 4,
        out_specs=[hbm] * 4,
        scratch_shapes=[pltpu.SemaphoreType.DMA((16,))],
        compiler_params=pltpu.CompilerParams(vmem_limit_bytes=8 * 2**20),
        name="write_out",
    )(*results)
    return (
        gt.reshape(1, 256, WIDTH),
        gq.reshape(1, 4096, 1, 128),
        gv.reshape(1, 4096, 1, 256),
        dw.reshape(128, WIDTH),
    )


def solution(mesh):
    return jax.shard_map(
        body,
        mesh=mesh,
        in_specs=(
            P("dp", "sp", None),
            P("dp", None),
            P("dp", None, "sp", None),
            P("dp", None, "sp", None),
            P("dp", "sp", None),
            P(),
        ),
        out_specs=(
            P("dp", "sp", None),
            P("dp", None, "sp", None),
            P("dp", None, "sp", None),
            P("dp", None),
        ),
        check_vma=False,
    )
```

```python
import functools

import jax
import jax.numpy as jnp
import numpy as np
from jax import lax
from jax.experimental import pallas as pl
from jax.experimental.pallas import tpu as pltpu
from jax.sharding import PartitionSpec as P

MESH = pl.DeviceIdType.MESH
F32, BF16 = jnp.float32, jnp.bfloat16
BLOCK = 128
NB = 32
WIDTH = 2048
CHAINS, CW = 3, 256
C1 = CHAINS * CW
C2 = WIDTH - C1
H2 = C2 // 2
ORDERS = {
    "cot": ((1, 1), (3, 3), (3, 1), (1, 3), (2, 1), (2, 3), (1, 2), (3, 2), (2, 2), (1, 0), (3, 0), (0, 2), (2, 0), (0, 1), (0, 3), (0, 0)),
    "gk": ((1, 1), (3, 3), (3, 1), (1, 3), (2, 1), (2, 3), (1, 2), (3, 2), (2, 2), (1, 0), (3, 0), (0, 2), (2, 0), (0, 1), (0, 3), (0, 0)),
    "end": ((2, 2), (1, 2), (3, 2), (2, 1), (2, 3), (0, 2), (1, 1), (1, 3), (3, 1), (3, 3), (2, 0), (0, 1), (0, 3), (1, 0), (3, 0), (0, 0)),
}
FACTOR = BLOCK**-0.5


def tables():
    half = 64
    freq = 10000.0 ** (-np.arange(half, dtype=np.float64) / half)
    freq = np.concatenate([freq, freq])
    sign = np.where(np.arange(128) < half, -1.0, 1.0)
    ang_j = np.arange(128, dtype=np.float64)[:, None] * freq
    ang_n = 128.0 * np.arange(NB, dtype=np.float64)[:, None] * freq
    inside = np.stack([np.cos(ang_j), np.sin(ang_j), sign * np.cos(ang_j), sign * np.sin(ang_j)])
    across = np.stack([np.cos(ang_n), np.sin(ang_n)], axis=1)
    return inside.astype(np.float32), across.astype(np.float32)


def dot(a, b, ca, cb):
    return lax.dot_general(a, b, (((ca,), (cb,)), ((), ())), preferred_element_type=F32)


TARGETS = (
    ((2, 2), (0, 2), (1, 2), (3, 0), (1, 0), (3, 2), (2, 0), (0, 0)),
    ((2, 1), (0, 3), (1, 3), (3, 1), (1, 1), (3, 3), (2, 3), (0, 1)),
)

SCRATCH = dict(
    tok=((512, WIDTH), BF16),
    wall=((8, 128, WIDTH), BF16),
    vv=((NB, 128, 256), BF16),
    rq=((NB, 128, 128), BF16),
    dq=((NB, 128, 128), BF16),
    cosv=((NB, 128, 128), F32),
    sinv=((NB, 128, 128), F32),
    jtv=((4, 128, 128), F32),
    ntv=((NB, 2, 128), F32),
    within=((128, 128), F32),
    rise=((128, 128), F32),
    fall=((128, 128), F32),
    cot=((NB, 128, 256), BF16),
    mix=((NB, 128, 128), BF16),
    trl=((NB, 128, 256), F32),
    trb=((NB, 128, 256), BF16),
    entb=((NB, 128, 256), BF16),
    gko=((NB, 128, 128), BF16),
    gki=((4, 128, 1024), BF16),
    gkt=((1024, 512), BF16),
    keyo=((8, 4, 128, 128), BF16),
    keyi=((NB, 128, 128), BF16),
    gts=((256, WIDTH), BF16),
    gtr=((256, WIDTH), BF16),
    dwz=((8, 128, C1), BF16),
    rz=((CHAINS, 2, 4, 128, CW), BF16),
    dwx=((2, 4, 4, 8, 8, H2), BF16),
    f1=((2, 2, 2, 8, 8, H2), BF16),
    r1=((2, 2, 4, 8, 8, H2), BF16),
    s1=((2, 4, 8, 8, H2), BF16),
    r2=((2, 4, 8, 8, H2), BF16),
    zx=((2, 8, 8, H2), BF16),
    zr=((2, 8, 8, H2), BF16),
    px=((16, 8, C1), BF16),
    pr=((16, 8, C1), BF16),
    fin=((16, 8, WIDTH), BF16),
)
SEMS = dict(
    loc=7, cot_s=1, cot_r=16, tok_s=1, tok_r=1, w_s=1, wp_r=7, wm_r=7, gk_s=2, gk_r=1, key_s=2, key_r=8,
    gt_s=1, gt_r=1, rz_s=1, rz_r=8 * CHAINS, f1_r=4, r1_s=1, r1_r=2, r2_s=1, r2_r=2, zx_s=1, zx_r=2, px_s=1, px_r=1, fin_s=1, finx_r=2, finz_r=1,
)


def kernel(ld_ref, jt_ref, nt_ref, tok_ref, w_ref, q_ref, v_ref, cot_ref, gt_o, gq_o, gv_o, dw_o, *scratch):
    B = type("B", (), dict(zip([*SCRATCH, *SEMS, "lds"], scratch, strict=True)))
    sp, dp = lax.axis_index("sp"), lax.axis_index("dp")
    y, x = lax.div(sp, 4), lax.rem(sp, 4)
    z, c = lax.div(dp, 2), lax.rem(dp, 2)
    head_core = lax.rem(x, 2)
    head_at = lax.div(sp, 2)

    def plane(t, name="end"):
        if isinstance(t, int):
            dy, dx = ORDERS[name][t]
        else:
            code = jnp.int32(0)
            for k, (a, b) in enumerate(ORDERS[name][:15]):
                code = jnp.where(t == k, a * 4 + b, code)
            dy, dx = lax.div(code, 4), lax.rem(code, 4)
        to = lax.rem(y + dy, 4) * 4 + lax.rem(x + dx, 4)
        of = lax.rem(y + 4 - dy, 4) * 4 + lax.rem(x + 4 - dx, 4)
        return to, of

    def zat(dz):
        return lax.rem(z + 8 + dz, 8)

    def zdev(dz, core=c):
        return zat(dz) * 2 + core

    def remote(src, dst, ss, rs, dev):
        return pltpu.make_async_remote_copy(
            src_ref=src, dst_ref=dst, send_sem=ss, recv_sem=rs, device_id=dev, device_id_type=MESH
        )

    def arrived(ref, sem):
        pltpu.make_async_copy(ref, ref, sem).wait()

    def loop(lo, hi, f):
        def step(i, carry):
            f(i)
            return carry

        lax.fori_loop(lo, hi, step, 0)

    def lanes(i, width=128):
        return pl.ds(pl.multiple_of(i * width, width), width)

    bar = pltpu.get_barrier_semaphore()
    partner = (sp, zdev(0, 1 - c))

    def greet(k):
        for core in (c, 1 - c):
            pl.semaphore_signal(bar, inc=1, device_id=(lax.rem(sp + k, 16), zdev(0, core)), device_id_type=MESH)

    loop(1, 16, greet)
    pl.semaphore_signal(bar, inc=1, device_id=partner, device_id_type=MESH)
    loop(1, 8, lambda k: pl.semaphore_signal(bar, inc=1, device_id=(sp, zdev(k)), device_id_type=MESH))

    loads = [
        pltpu.make_async_copy(ld_ref, B.lds, B.loc.at[6]),
        pltpu.make_async_copy(q_ref, B.rq, B.loc.at[0]),
        pltpu.make_async_copy(v_ref, B.vv, B.loc.at[1]),
        pltpu.make_async_copy(tok_ref, B.tok.at[pl.ds(c * 256, 256)], B.loc.at[2]),
        pltpu.make_async_copy(w_ref, B.wall.at[z], B.loc.at[3]),
        pltpu.make_async_copy(jt_ref, B.jtv, B.loc.at[4]),
        pltpu.make_async_copy(nt_ref, B.ntv, B.loc.at[5]),
        pltpu.make_async_copy(cot_ref.at[:, :, lanes(sp, 256)], B.cot.at[pl.ds(2 * sp, 2)], B.cot_r.at[sp]),
    ]
    for cp in loads:
        cp.start()
    pl.semaphore_wait(bar, 38)

    up, down = (sp, zdev(1)), (sp, zdev(-1))

    def w_copy(k, part, way):
        at = zat(-k if way == 0 else k)
        rows = pl.ds(64 * part, 64)
        sem = (B.wp_r if way == 0 else B.wm_r).at[2 * k + part if k < 3 else 6]
        src = w_ref.at[rows] if k == 0 else B.wall.at[at, rows]
        return remote(src, B.wall.at[at, rows], B.w_s.at[0], sem, up if way == 0 else down)

    def w_step(k, part):
        for way in (0, 1):
            if k == 4:
                arrived(B.wall.at[zat(4), pl.ds(64 * way, 64)], (B.wp_r, B.wm_r)[way].at[6])
                continue
            at = zat(-k if way == 0 else k)
            arrived(B.wall.at[at, pl.ds(64 * part, 64)], (B.wp_r, B.wm_r)[way].at[2 * (k - 1) + part])
            if k < 3 or part == way:
                w_copy(k, part, way).start()

    for part in range(2):
        for way in (0, 1):
            w_copy(0, part, way).start()

    def cot_copy(t):
        to, _ = plane(t, "cot")
        return remote(
            cot_ref.at[:, :, lanes(to, 256)], B.cot.at[pl.ds(2 * sp, 2)], B.cot_s.at[0], B.cot_r.at[sp], (to, dp)
        )

    for t in range(15):
        cot_copy(t).start()
    tok_copy = remote(tok_ref, B.tok.at[pl.ds(c * 256, 256)], B.tok_s.at[0], B.tok_r.at[0], partner)
    tok_copy.start()

    loads[0].wait()
    ld = B.lds[sp]
    rows = lax.broadcasted_iota(jnp.int32, (128, 128), 0).astype(F32)
    cols = lax.broadcasted_iota(jnp.int32, (128, 128), 1).astype(F32)
    offset = rows - cols
    B.within[...] = jnp.where(offset >= 0, jnp.exp(jnp.maximum(offset, 0.0) * ld), 0.0)
    B.rise[...] = jnp.exp((rows + 1.0) * ld)
    B.fall[...] = jnp.exp((127.0 - rows) * ld)
    growth = jnp.exp(jnp.full((1, 256), 128.0, F32) * ld)
    loads[5].wait()
    loads[6].wait()
    loads[1].wait()

    def turn(n):
        cn, sn = B.ntv[n, 0:1, :], B.ntv[n, 1:2, :]
        cosine = cn * B.jtv[0] - sn * B.jtv[1]
        sine = sn * B.jtv[2] + cn * B.jtv[3]
        B.cosv[n] = cosine
        B.sinv[n] = sine
        u = B.rq[n].astype(F32)
        r = (u * cosine + pltpu.roll(u, 64, 1) * sine).astype(BF16)
        B.rq[n] = r
        B.dq[n] = (r.astype(F32) * B.rise[...]).astype(BF16)

    loop(0, NB, turn)

    def keys(hh):
        def part(i):
            k = dot(B.tok[pl.ds(pl.multiple_of(i * 256, 256), 256), :], B.wall[hh], 1, 1)
            B.keyo[hh, pl.ds(2 * i, 2)] = k.astype(BF16).reshape(2, 128, 128)

        loop(0, 2, part)

    def key_copy(hh, i, sem, u):
        return remote(
            B.keyo.at[hh, pl.ds(2 * i, 2)],
            B.keyi.at[pl.ds(2 * sp, 2)],
            B.key_s.at[sem],
            B.key_r.at[u],
            (2 * hh + c, zdev(0, i)),
        )

    own_head_here = head_core == c

    def key_send(hh, u):
        for i in range(2):
            special = jnp.logical_and(hh == head_at, c == i)

            @pl.when(jnp.logical_and(special, own_head_here))
            def _():
                pltpu.make_async_copy(
                    B.keyo.at[hh, pl.ds(2 * i, 2)], B.keyi.at[pl.ds(2 * sp, 2)], B.key_r.at[u]
                ).start()

            @pl.when(jnp.logical_and(special, jnp.logical_not(own_head_here)))
            def _():
                key_copy(hh, i, 1, u).start()

            @pl.when(jnp.logical_not(special))
            def _():
                key_copy(hh, i, 0, u).start()

    def cot_chunk(t):
        _, p = plane(t, "cot")
        arrived(B.cot.at[pl.ds(2 * p, 2)], B.cot_r.at[p])
        for b in range(2):
            n = 2 * p + b
            cb = B.cot[n]
            m = dot(cb, B.vv[n], 1, 1) * B.within[...]
            B.mix[n] = m.astype(BF16)
            B.trl[n] = dot(B.dq[n], cb, 0, 0)

    def take_tokens():
        loads[3].wait()
        arrived(B.tok.at[pl.ds((1 - c) * 256, 256)], B.tok_r.at[0])
        loads[4].wait()
        loads[2].wait()

    def keys_of(first, step, count):
        loop(0, count, lambda i: keys(zat(first + step * i)))

    def mixing(lo, hi):
        loop(lo, hi, cot_chunk)

    def scan(i, carry):
        n = NB - 1 - i
        B.trb[n] = carry.astype(BF16)
        return B.trl[n] + growth * carry

    def trails():
        lax.fori_loop(0, NB, scan, jnp.zeros((128, 256), F32))

    def gk_copy(t, sem=0):
        to, _ = plane(t, "gk")
        return remote(
            B.gko.at[pl.ds(2 * to, 2)],
            B.gki.at[pl.ds(2 * c, 2), :, lanes(head_at)],
            B.gk_s.at[sem],
            B.gk_r.at[0],
            (to, zdev(0, head_core)),
        )

    def gk_chunk(t):
        p, _ = plane(t, "gk")
        for b in range(2):
            n = 2 * p + b
            g = dot(B.mix[n], B.rq[n], 0, 0) + B.fall[...] * dot(B.vv[n], B.trb[n], 1, 1)
            g = g * B.cosv[n] - pltpu.roll(g, 64, 1) * B.sinv[n]
            B.gko[n] = (g * FACTOR).astype(BF16)

        @pl.when(t < 15)
        def _():
            gk_copy(t).start()

    def key_grads(lo, hi):
        loop(lo, hi, gk_chunk)
        if hi < 16:
            return

        @pl.when(own_head_here)
        def _():
            pltpu.make_async_copy(
                B.gko.at[pl.ds(2 * sp, 2)], B.gki.at[pl.ds(2 * c, 2), :, lanes(head_at)], B.gk_r.at[0]
            ).start()

        @pl.when(jnp.logical_not(own_head_here))
        def _():
            gk_copy(15, 1).start()

    def take_key_grads():
        arrived(B.gki, B.gk_r.at[0])
        for i in range(4):
            B.gkt[:, 128 * i : 128 * i + 128] = B.gki[i].T

    def send_keys(lo, hi):
        even = lax.rem(x + c, 2) == 0
        for u in range(lo, hi):
            (y0, x0), (y1, x1) = TARGETS[0][u], TARGETS[1][u]
            to = lax.rem(y + jnp.where(even, y0, y1), 4) * 4 + lax.rem(x + jnp.where(even, x0, x1), 4)
            key_send(lax.div(to, 2), u)

    def ring_refs(chain, way, k):
        at = pl.ds(chain * CW, CW)
        return at, B.rz.at[chain, way, k - 1], B.rz_r.at[(chain * 2 + way) * 4 + k - 1]

    def ring_send(chain, way, k):
        at, dst, sem = ring_refs(chain, way, k)
        d = zat(k if way == 0 else -k)
        remote(B.dwz.at[d, :, at], dst, B.rz_s.at[0], sem, up if way == 0 else down).start()

    def ring_take(chain, way, k):
        at, got, sem = ring_refs(chain, way, k)
        arrived(got, sem)
        if k == 1:
            return
        d = zat(k - 1 if way == 0 else 1 - k)

        def add(i):
            r = pl.ds(pl.multiple_of(i * 32, 32), 32)
            B.dwz[d, r, at] = (B.dwz[d, r, at].astype(F32) + got[r, :].astype(F32)).astype(BF16)

        loop(0, 4, add)
        ring_send(chain, way, k - 1)

    def take(chain, k):
        ring_take(chain, chain % 2, k)
        if k > 1:
            ring_take(chain, 1 - chain % 2, k - 1)

    def weight_ring(lo, hi):
        def tile(i):
            g = dot(B.gkt[...], B.tok[:, lanes(i, CW)], 1, 0)
            B.dwz[:, :, lanes(i, CW)] = g.astype(BF16).reshape(8, 128, CW)

        loop(lo, hi, tile)
        for chain in range(lo, hi):
            ring_send(chain, chain % 2, 4)
            ring_send(chain, 1 - chain % 2, 3)

    def line(way, step):
        if way == 0:
            at = lax.rem(x + step, 4)
            return at, x, (y * 4 + at, dp)
        at = lax.rem(y + step, 4)
        return at, y, (at * 4 + x, dp)

    def weight_plane(way):
        def tile(at, width):
            g = dot(B.gkt[...], B.tok[:, pl.ds(C1 + way * H2 + at, width)], 1, 0)
            g = g.astype(BF16).reshape(8, 4, 4, 8, width)
            for yy in range(4):
                for xx in range(4):
                    a1, a2 = (xx, yy) if way == 0 else (yy, xx)
                    B.dwx[way, a1, a2, :, :, pl.ds(at, width)] = g[:, yy, xx]

        if H2 % 256 == 0:
            loop(0, H2 // 256, lambda i: tile(pl.multiple_of(i * 256, 256), 256))
        else:
            for at in range(0, H2, 256):
                tile(at, min(256, H2 - at))
        for step in (1, 3):
            near, _, dev = line(way, step)
            far, _, _ = line(way, 2)
            side = 0 if step == 1 else 1
            through, own = pl.ds(2 * side, 2), pl.ds(2 - 2 * side, 2)
            remote(B.dwx.at[way, far, through], B.f1.at[way, side], B.r1_s.at[0], B.f1_r.at[2 * way + side], dev).start()
            remote(B.dwx.at[way, near, own], B.r1.at[way, side, own], B.r1_s.at[0], B.r1_r.at[way], dev).start()

    def line_pass(way):
        for step in (1, 3):
            near, _, dev = line(way, step)
            side = 0 if step == 1 else 1
            arrived(B.f1.at[way, side], B.f1_r.at[2 * way + side])

            def add(i):
                j, hh = lax.div(i, 4), lax.rem(i, 4) * 2
                have = B.dwx[way, near, 2 * side + j, pl.ds(hh, 2)].astype(F32)
                B.dwx[way, near, 2 * side + j, pl.ds(hh, 2)] = (have + B.f1[way, side, j, pl.ds(hh, 2)].astype(F32)).astype(BF16)

            loop(0, 8, add)
            through = pl.ds(2 * side, 2)
            remote(
                B.dwx.at[way, near, through], B.r1.at[way, side, through], B.r1_s.at[0], B.r1_r.at[way], dev
            ).start()

    def line_sums(way):
        arrived(B.r1.at[way], B.r1_r.at[way])
        me = (x, y)[way]

        def add(i):
            j, hh = lax.div(i, 4), lax.rem(i, 4) * 2
            total = B.dwx[way, me, j, pl.ds(hh, 2)].astype(F32)
            for side in range(2):
                total += B.r1[way, side, j, pl.ds(hh, 2)].astype(F32)
            B.s1[way, j, pl.ds(hh, 2)] = total.astype(BF16)

        loop(0, 16, add)
        for step in (2, 1, 3):
            at, here, dev = line(1 - way, step)
            remote(B.s1.at[way, at], B.r2.at[way, here], B.r2_s.at[0], B.r2_r.at[way], dev).start()

    def plane_sums(way):
        arrived(B.r2.at[way, 0:3], B.r2_r.at[way])
        B.r2[way, (y, x)[way]] = B.s1[way, (y, x)[way]]
        for hh in range(8):
            total = B.r2[way, 0, hh].astype(F32)
            for p in range(1, 4):
                total += B.r2[way, p, hh].astype(F32)
            B.zx[way, hh] = total.astype(BF16)
        for k in (4, 3, 5, 2, 6, 1, 7):
            d = zat(k)
            remote(B.zx.at[way, d], B.zr.at[way, z], B.zx_s.at[0], B.zx_r.at[way], (sp, zdev(k))).start()

    def own_rows(i):
        r = pl.ds(pl.multiple_of(i * 16, 16), 16)
        for chain in range(CHAINS):
            at = slice(chain * CW, chain * CW + CW)
            v = B.dwz[z, r, at].astype(F32) + B.rz[chain, 0, 0, r, :].astype(F32) + B.rz[chain, 1, 0, r, :].astype(F32)
            B.px[pl.ds(2 * i, 2), :, at] = v.reshape(2, 8, CW).astype(BF16)

    def column_sums():
        loop(0, 8, own_rows)
        for t in range(15):
            to, _ = plane(t)
            remote(B.px.at[to], B.pr.at[sp], B.px_s.at[0], B.px_r.at[0], (to, dp)).start()

    def total_of(ref, count):
        total = ref[0].astype(F32)
        for p in range(1, count):
            total += ref[p].astype(F32)
        return total.astype(BF16)

    def fin_send(lo, hi, sem):
        for t in range(15):
            to, _ = plane(t)
            ref = B.fin.at[sp, :, pl.ds(lo, hi - lo)]
            remote(ref, ref, B.fin_s.at[0], sem, (to, dp)).start()

    def finish_plane_part(way):
        arrived(B.zr.at[way, 0:7], B.zx_r.at[way])
        B.zr[way, z] = B.zx[way, z]
        lo = C1 + way * H2
        B.fin[sp, :, lo : lo + H2] = total_of(B.zr.at[way], 8)
        fin_send(lo, lo + H2, B.finx_r.at[way])

    def finish_ring_part():
        B.pr[sp] = B.px[sp]
        arrived(B.pr.at[0:15], B.px_r.at[0])
        B.fin[sp, :, 0:C1] = total_of(B.pr, 16)
        fin_send(0, C1, B.finz_r.at[0])

    def widen(j):
        dw_o[j] = B.fin[j].astype(F32)

    def weight_out():
        for way in (0, 1):
            arrived(B.fin.at[0:15, :, C1 + way * H2 : C1 + way * H2 + H2], B.finx_r.at[way])
        arrived(B.fin.at[0:15, :, 0:C1], B.finz_r.at[0])
        loop(0, 16, widen)

    def gt_tile(first):
        def tile(i):
            j = (1 - c) if first else c
            a = jnp.concatenate([B.gki[2 * j], B.gki[2 * j + 1]], axis=0)
            g = dot(a, B.wall[:, :, lanes(i, 256)].reshape(1024, 256), 1, 0)
            if first:
                B.gts[:, lanes(i, 256)] = g.astype(BF16)
            else:
                gt_o[:, lanes(i, 256)] = (g + B.gtr[:, lanes(i, 256)].astype(F32)).astype(BF16)

        return tile

    gt_copy = remote(B.gts, B.gtr, B.gt_s.at[0], B.gt_r.at[0], partner)

    def token_grads_partner(lo, hi):
        loop(lo, hi, gt_tile(True))
        if hi == 8:
            gt_copy.start()

    def token_grads(lo, hi):
        if lo == 0:
            arrived(B.gtr, B.gt_r.at[0])
        loop(lo, hi, gt_tile(False))

    def back_a(u):
        arrived(B.keyi.at[0:4], B.key_r.at[u])
        for cls in range(2):
            code = jnp.int32(0)
            for k, (dy, dx) in enumerate(TARGETS[cls]):
                code = jnp.where(u == k, (4 - dy) % 4 * 4 + (4 - dx) % 4, code)
            p = lax.rem(y + lax.div(code, 4), 4) * 4 + lax.rem(x + lax.rem(code, 4), 4)
            for b in range(2):
                n = 2 * p + b
                k0 = B.keyi[n].astype(F32)
                rk = ((k0 * B.cosv[n] + pltpu.roll(k0, 64, 1) * B.sinv[n]) * FACTOR).astype(BF16)
                B.keyi[n] = rk
                B.dq[n] = (dot(B.rq[n], rk, 1, 1) * B.within[...]).astype(BF16)
                dk = (rk.astype(F32) * B.fall[...]).astype(BF16)
                B.trl[n] = dot(dk, B.vv[n], 0, 0)

    def scan_up(n, carry):
        B.entb[n] = carry.astype(BF16)
        return B.trl[n] + growth * carry

    def back_c(i):
        for b in range(4):
            n = 4 * i + b
            rk, cb, f = B.keyi[n], B.cot[n], B.fall[...]
            g = dot(B.mix[n], rk, 1, 0) + B.rise[...] * dot(cb, B.entb[n], 1, 1)
            gq_o[n] = (g * B.cosv[n] - pltpu.roll(g, 64, 1) * B.sinv[n]).astype(BF16)
            near, far = dot(B.dq[n], cb, 0, 0), dot(rk, B.trb[n], 1, 0)
            for h in range(2):
                at = slice(128 * h, 128 * h + 128)
                gv_o[n, :, at] = (near[:, at] + f * far[:, at]).astype(BF16)

    def scores(lo, hi):
        loop(lo, hi, back_a)

    def states():
        lax.fori_loop(0, NB, scan_up, jnp.zeros((128, 256), F32))

    def query_value_grads(lo, hi):
        loop(lo, hi, back_c)

    SCHEDULE = (
        (take_tokens,),
        (keys_of, 0, 1, 1),
        (w_step, 1, 0),
        (mixing, 0, 3),
        (w_step, 1, 1),
        (keys_of, -1, 2, 2),
        (mixing, 3, 7),
        (w_step, 2, 0),
        (mixing, 7, 12),
        (w_step, 2, 1),
        (mixing, 12, 16),
        (trails,),
        (key_grads, 0, 8),
        (w_step, 3, 0),
        (key_grads, 8, 16),
        (w_step, 3, 1),
        (keys_of, -3, 1, 2),
        (keys_of, 2, 1, 2),
        (take_key_grads,),
        (weight_plane, 0),
        (weight_ring, 0, 2),
        (weight_plane, 1),
        (weight_ring, 2, 3),
        (w_step, 4, 0),
        (keys_of, 4, 1, 1),
        (token_grads_partner, 0, 5),
        (take, 0, 4),
        (line_pass, 0),
        (take, 1, 4),
        (line_pass, 1),
        (take, 2, 4),
        (send_keys, 0, 1),
        (send_keys, 1, 2),
        (token_grads_partner, 5, 8),
        (take, 0, 3),
        (take, 1, 3),
        (take, 2, 3),
        (line_sums, 0),
        (send_keys, 2, 3),
        (send_keys, 3, 4),
        (take, 0, 2),
        (take, 1, 2),
        (take, 2, 2),
        (line_sums, 1),
        (send_keys, 4, 5),
        (send_keys, 5, 6),
        (take, 0, 1),
        (token_grads, 0, 3),
        (take, 1, 1),
        (take, 2, 1),
        (column_sums,),
        (send_keys, 6, 7),
        (send_keys, 7, 8),
        (scores, 0, 2),
        (plane_sums, 0),
        (scores, 2, 3),
        (plane_sums, 1),
        (token_grads, 3, 6),
        (finish_ring_part,),
        (scores, 3, 4),
        (finish_plane_part, 0),
        (scores, 4, 5),
        (finish_plane_part, 1),
        (scores, 5, 8),
        (states,),
        (token_grads, 6, 8),
        (query_value_grads, 0, 8),
        (weight_out,),
    )
    for step in SCHEDULE:
        step[0](*step[1:])

    arrived(B.cot.at[0:30], B.cot_s.at[0])
    arrived(B.wall.at[0:7], B.w_s.at[0])
    tok_copy.wait_send()
    gt_copy.wait_send()
    arrived(B.gko.at[0:30], B.gk_s.at[0])
    arrived(B.keyi.at[0:30], B.key_s.at[0])

    @pl.when(jnp.logical_not(own_head_here))
    def _():
        arrived(B.gko.at[0:2], B.gk_s.at[1])
        arrived(B.keyi.at[0:2], B.key_s.at[1])

    arrived(B.dwz.at[0:7], B.rz_s.at[0])
    arrived(B.dwx.at[:, 0:3], B.r1_s.at[0])
    arrived(B.s1.at[:, 0:3], B.r2_s.at[0])
    arrived(B.px.at[0:15], B.px_s.at[0])
    arrived(B.zx.at[:, 0:7], B.zx_s.at[0])
    arrived(B.fin.at[0:15], B.fin_s.at[0])


def write_out(*refs):
    ins, outs, sems = refs[:4], refs[4:8], refs[8]
    copies = []
    for a, b in zip(ins, outs, strict=True):
        rows = a.shape[0] // 4
        for i in range(4):
            at = pl.ds(i * rows, rows)
            copies.append(pltpu.make_async_copy(a.at[at], b.at[at], sems.at[len(copies)]))
    for cp in copies:
        cp.start()
    for cp in copies:
        cp.wait()


def body(tokens, key_weight, queries, values, cotangent, log_decay):
    inside, across = tables()
    hbm, vmem = pl.BlockSpec(memory_space=pltpu.HBM), pl.BlockSpec(memory_space=pltpu.VMEM)
    shapes = [
        jax.ShapeDtypeStruct((256, WIDTH), BF16),
        jax.ShapeDtypeStruct((NB, 128, 128), BF16),
        jax.ShapeDtypeStruct((NB, 128, 256), BF16),
        jax.ShapeDtypeStruct((16, 8, WIDTH), F32),
    ]
    results = pl.pallas_call(
        kernel,
        out_shape=shapes,
        in_specs=[hbm] * 8,
        out_specs=[vmem] * 4,
        scratch_shapes=[pltpu.VMEM(shape, kind) for shape, kind in SCRATCH.values()]
        + [pltpu.SemaphoreType.DMA((n,)) for n in SEMS.values()]
        + [pltpu.SMEM((16,), F32)],
        compiler_params=pltpu.CompilerParams(
            collective_id=0, has_side_effects=True, vmem_limit_bytes=48 * 2**20
        ),
        name="retention",
    )(
        *(
            pltpu.with_memory_space_constraint(a, pltpu.HBM)
            for a in (
                log_decay,
                jnp.asarray(inside),
                jnp.asarray(across),
                tokens.reshape(256, WIDTH),
                key_weight,
                queries.reshape(NB, 128, 128),
                values.reshape(NB, 128, 256),
                cotangent.reshape(2, 128, 4096),
            )
        ),
    )
    gt, gq, gv, dw = pl.pallas_call(
        write_out,
        out_shape=shapes,
        in_specs=[vmem] * 4,
        out_specs=[hbm] * 4,
        scratch_shapes=[pltpu.SemaphoreType.DMA((16,))],
        compiler_params=pltpu.CompilerParams(vmem_limit_bytes=8 * 2**20),
        name="write_out",
    )(*results)
    return (
        gt.reshape(1, 256, WIDTH),
        gq.reshape(1, 4096, 1, 128),
        gv.reshape(1, 4096, 1, 256),
        dw.reshape(128, WIDTH),
    )


def solution(mesh):
    return jax.shard_map(
        body,
        mesh=mesh,
        in_specs=(
            P("dp", "sp", None),
            P("dp", None),
            P("dp", None, "sp", None),
            P("dp", None, "sp", None),
            P("dp", "sp", None),
            P(),
        ),
        out_specs=(
            P("dp", "sp", None),
            P("dp", None, "sp", None),
            P("dp", None, "sp", None),
            P("dp", None),
        ),
        check_vma=False,
    )
```
